512 devices in a mesh: grp: 2 (over y), sp: 64 (over z, core), tp: 4 (over x).
Axes of the slice: x: 4, y: 2, z: 32, core: 2. Of those that a mesh axis runs over, the one named last changes fastest.
The devices are a block of a 4x8x32 slice.
Arguments:
- tokens: bfloat16 [131072, 2048], P(('grp', 'sp', 'tp')), parts along dimension 0, may hold values from -6 to 6
- step: float32 [131072], P(('grp', 'sp')), parts along dimension 0, may hold values from 0.2 to 3.75
- in_gain: float32 [2048], replicated, may hold values from 0.1 to 1.9
- in_proj: bfloat16 [2048, 512], P(None, 'tp'), may hold values from -0.125 to 0.125
- decay_rate: float32 [32, 64], P('tp'), may hold values from 1.5258789e-06 to 0.04
- frequency: float32 [32, 64], P('tp'), may hold values from 0.2 to 3
- input_map: float32 [2, 32, 64, 16], P(None, 'tp'), may hold values from -1 to 1
- readout: float32 [2, 32, 16, 64], P(None, 'tp'), may hold values from -0.75 to 0.75
- out_gain: float32 [512], replicated, may hold values from 0.1 to 1.9
- out_proj: bfloat16 [512, 2048], replicated, may hold values from -0.25 to 0.25
Outputs:
- mixed: bfloat16 [131072, 2048], P(('grp', 'sp', 'tp')), parts along dimension 0
The draws below stay inside these ranges and needn't reach their ends.
There are 2 independent parts, one for each index of `grp`. The reference program is written for one: setup_inputs(seed, part) draws one part's arguments, and reference() takes and returns one part's arrays. A program takes and returns all parts, laid end to end along the dimension named above; an argument that names none is the same for every part. Nothing has to cross between parts.
All inputs are finite; a program needn't handle non-finite values.
Results may differ from the reference program's by a relative error of at most 0.01.
Values may be sent and summed in bfloat16 or wider, within the bound.
A program may use at most 64 MiB of HBM per device.

```python
import jax
import jax.numpy as jnp
from jax import lax

D = 2048
CHANNELS = 512
GROUP_CH = 16
STATE = 64
GROUPS = 32
SEQ_DEV = 1024
TOKENS = 65536


def draw_step(key, part):
    level_key, fine_key = jax.random.split(key)
    levels = jnp.exp(jax.random.uniform(level_key, (TOKENS // SEQ_DEV,), jnp.float32, jnp.log(0.4), jnp.log(2.5)))
    fine = jnp.clip(1.0 + 0.25 * jax.random.normal(fine_key, (TOKENS,), jnp.float32), 0.5, 1.5)
    return jnp.repeat(levels, SEQ_DEV, total_repeat_length=TOKENS) * fine


def draw_decay_rate(key, part):
    pick_key, slow_key, fast_key = jax.random.split(key, 3)
    share = 0.5
    slow_mask = jax.random.uniform(pick_key, (GROUPS, STATE), jnp.float32) < share
    slow = jnp.exp(jax.random.uniform(slow_key, (GROUPS, STATE), jnp.float32, jnp.log(0.1), 0.0)) / TOKENS
    fast = jnp.exp(jax.random.uniform(fast_key, (GROUPS, STATE), jnp.float32, jnp.log(0.01), jnp.log(0.04)))
    return jnp.where(slow_mask, slow, fast)


def block_scale(rng, shape, pieces, low, top_value):
    factor_of, own = 1.0, jax.random.fold_in(rng, 6)
    for dim, blocks in pieces:
        heights = jnp.exp(jax.random.uniform(jax.random.fold_in(own, dim), (blocks,), jnp.float32, low / len(pieces), top_value / len(pieces)))
        factor_of = factor_of * jnp.repeat(heights, shape[dim] // blocks).reshape([-1 if axis == dim else 1 for axis in range(len(shape))])
    return factor_of


def gaussian(rng, shape, deviation, limit, cuts=(), kind=jnp.bfloat16):
    drawn = jax.random.normal(rng, shape, jnp.float32) * deviation
    if len(cuts) > 0:
        drawn = block_scale(rng, shape, cuts, -0.22, 0.18) * drawn
    return jnp.clip(drawn, min=-limit, max=limit).astype(kind)


def setup_inputs(seed: int = 0, part: int = 0) -> dict:
    splits = jax.random.split(jax.random.key(seed), 11)
    part_splits = jax.random.split(jax.random.fold_in(splits[10], part), 11)
    return {
        "tokens": gaussian(part_splits[0], (TOKENS, D), 1.0, 6.0, ((0, 256),)),
        "step": draw_step(jax.random.fold_in(jax.random.fold_in(splits[10], part), 71), part),
        "in_gain": jnp.clip(1.0 + 0.18 * jax.random.normal(splits[2], (D,), jnp.float32), 0.1, 1.9),
        "in_proj": gaussian(splits[3], (D, CHANNELS), D ** -0.5, 0.125, ((1, 4),)),
        "decay_rate": draw_decay_rate(jax.random.fold_in(splits[10], 71), part),
        "frequency": jnp.clip(0.2 + 2.8 * jax.random.uniform(splits[5], (GROUPS, STATE), jnp.float32) ** block_scale(splits[5], (GROUPS, STATE), ((0, 4),), -0.2, 0.2), 0.2, 3.0),
        "input_map": gaussian(splits[6], (2, GROUPS, STATE, GROUP_CH), (2 * GROUP_CH) ** -0.5, 1.0, ((1, 4),), jnp.float32),
        "readout": gaussian(splits[7], (2, GROUPS, GROUP_CH, STATE), STATE ** -0.5, 0.75, ((1, 4),), jnp.float32),
        "out_gain": jnp.clip(1.0 + 0.18 * jax.random.normal(splits[8], (CHANNELS,), jnp.float32), 0.1, 1.9),
        "out_proj": gaussian(splits[9], (CHANNELS, D), CHANNELS ** -0.5, 0.25),
    }


HIGHEST = lax.Precision.HIGHEST

def compose(earlier, later):
    a_re, a_im, b_re, b_im = earlier
    c_re, c_im, d_re, d_im = later
    return (c_re * a_re - c_im * a_im, c_re * a_im + c_im * a_re, c_re * b_re - c_im * b_im + d_re, c_re * b_im + c_im * b_re + d_im)

def rms_rows(values, gain):
    values = values.astype(jnp.float32)
    scaled = values * lax.rsqrt(lax.optimization_barrier(jnp.mean(values * values, axis=-1, keepdims=True)) + 1e-06)
    return (scaled * gain).astype(jnp.bfloat16)

def transition(times, decay_rate, frequency):
    spans = times.astype(jnp.float32)[:, None, None]
    magnitude = jnp.exp(-decay_rate[None] * spans)
    a_re = magnitude * jnp.cos(frequency[None] * spans)
    a_im = magnitude * jnp.sin(frequency[None] * spans)
    lam_re = -decay_rate
    denom = lam_re * lam_re + frequency * frequency
    n_re = a_re - 1.0
    z_re = (n_re * lam_re + a_im * frequency) / denom
    z_im = (a_im * lam_re - n_re * frequency) / denom
    return (a_re, a_im, z_re, z_im)

def injection(drive, input_map, z_re, z_im):
    groups = input_map.shape[1]
    grouped = drive.astype(jnp.float32).reshape(drive.shape[0], groups, -1)
    push_re = jnp.einsum('tgh,gph->tgp', grouped, input_map[0], precision=HIGHEST)
    push_im = jnp.einsum('tgh,gph->tgp', grouped, input_map[1], precision=HIGHEST)
    return (z_re * push_re - z_im * push_im, z_re * push_im + z_im * push_re)

def response(s_re, s_im, readout):
    value = jnp.einsum('tgp,ghp->tgh', s_re, readout[0], precision=HIGHEST) - jnp.einsum('tgp,ghp->tgh', s_im, readout[1], precision=HIGHEST)
    value = value.reshape(s_re.shape[0], -1)
    return jax.nn.gelu(value, approximate=True).astype(jnp.bfloat16)

def reference(tokens, step, in_gain, in_proj, decay_rate, frequency, input_map, readout, out_gain, out_proj):
    normed = rms_rows(tokens, in_gain)
    drive = jnp.dot(normed, in_proj, preferred_element_type=jnp.float32).astype(jnp.bfloat16)
    block_count = TOKENS // SEQ_DEV
    drive_blocks = drive.reshape(block_count, SEQ_DEV, -1)
    time_blocks = step.reshape(block_count, SEQ_DEV)
    zero = jnp.zeros(decay_rate.shape, jnp.float32)

    def advance(carry, piece):
        drive_part, time_part = piece
        a_re, a_im, z_re, z_im = transition(time_part, decay_rate, frequency)
        i_re, i_im = injection(drive_part, input_map, z_re, z_im)
        c_re, c_im, s_re, s_im = lax.associative_scan(compose, (a_re, a_im, i_re, i_im), axis=0)
        s_re = s_re + c_re * carry[0] - c_im * carry[1]
        s_im = s_im + c_re * carry[1] + c_im * carry[0]
        return ((s_re[-1], s_im[-1]), response(s_re, s_im, readout))
    _, answer = lax.scan(advance, (zero, zero), (drive_blocks, time_blocks))
    answer = answer.reshape(TOKENS, -1)
    shaped = rms_rows(answer, out_gain)
    return jnp.dot(shaped, out_proj, preferred_element_type=jnp.float32).astype(jnp.bfloat16)
```

```python
import functools

import jax
import jax.numpy as jnp
import numpy as np
from jax import lax
from jax.experimental import pallas as pl
from jax.experimental.pallas import tpu as pltpu
from jax.sharding import PartitionSpec as P

F32, BF16 = jnp.float32, jnp.bfloat16
MESH = pl.DeviceIdType.MESH
LANES = 128
CHUNK = 64
SIN = (6.283182782944718, -41.34141729070845, 81.59606953187966, -76.57887013158442, 41.19977042473147, -12.262090350994187)
COS = (0.9999999888727491, -19.7392044313539, 64.939113609812, -85.45006239525888, 60.16694808625918, -25.96486025322117, 6.5245930831162795)
TURN = np.float32(1.0 / (2.0 * np.pi))
TURN_LOW = np.float32(1.0 / (2.0 * np.pi) - float(TURN))


def halves(value):
    wide = value * np.float32(4097.0)
    high = wide - (wide - value)
    return high, value - high


def turns_of(freqs):
    high = freqs * TURN
    f_high, f_low = halves(freqs)
    c_high, c_low = (np.float32(v) for v in halves(TURN))
    error = ((f_high * c_high - high) + f_high * c_low + f_low * c_high) + f_low * c_low
    return high, error + freqs * TURN_LOW


def polynomial(x, terms):
    total = jnp.full_like(x, np.float32(terms[-1]))
    for term in terms[-2::-1]:
        total = total * x + np.float32(term)
    return total


def rotation(high, low, times):
    whole = high * times
    part = (whole - jnp.round(whole)) + low * times
    square = part * part
    return polynomial(square, COS), polynomial(square, SIN) * part


def gather_kernel(
    proj, tables, rates, step, all_proj, all_tables, all_rates, both_steps,
    proj_own, tables_own, rates_own, step_own, send, recv, small_send, small_recv, local,
):
    count = lax.axis_size("tp")
    me, sp = lax.axis_index("tp"), lax.axis_index("sp")
    core = lax.rem(sp, 2)
    partner = {"sp": sp + 1 - 2 * core}
    right, left = lax.rem(me + 1, count), lax.rem(me + count - 1, count)
    across = lax.rem(me + 2, count)
    to_right, to_left, to_across = {"tp": right}, {"tp": left}, {"tp": across}

    barrier = pltpu.get_barrier_semaphore()
    for target in (to_right, to_left, to_across, partner):
        pl.semaphore_signal(barrier, inc=1, device_id=target, device_id_type=MESH)

    inward = [
        pltpu.make_async_copy(src, dst, local.at[k])
        for k, (src, dst) in enumerate(
            ((proj, proj_own), (tables, tables_own), (rates, rates_own), (step, step_own))
        )
    ]
    for copy in inward:
        copy.start()
    for copy in inward:
        copy.wait()
    pl.semaphore_wait(barrier, 4)

    pairs = ((proj_own, all_proj), (tables_own, all_tables))

    def rows(k, quarter):
        quarter_rows = pairs[k][0].shape[0] // 4
        return pl.ds(pl.multiple_of((core * 2 + quarter) * quarter_rows, quarter_rows), quarter_rows)

    def remote(src, dst, slot, target):
        return pltpu.make_async_remote_copy(
            src_ref=src, dst_ref=dst, send_sem=send.at[slot], recv_sem=recv.at[slot],
            device_id=target, device_id_type=MESH,
        )

    def piece(k, shard, quarter, slot, target, own=False):
        own_ref, all_ref = pairs[k]
        where = rows(k, quarter)
        dst = all_ref.at[shard, where]
        return remote(own_ref.at[where] if own else dst, dst, slot, target)

    started = []

    def go(copy):
        copy.start()
        started.append(copy)

    for order in range(2):
        for k in (1, 0):
            go(piece(k, me, order, k * 12 + order, to_right, own=True))
            go(piece(k, me, 1 - order, k * 12 + 2 + order, to_left, own=True))
    small = []
    for slot, target in enumerate((to_right, to_left, to_across)):
        small.append(
            pltpu.make_async_remote_copy(
                src_ref=rates_own, dst_ref=all_rates.at[me], send_sem=small_send.at[slot],
                recv_sem=small_recv.at[slot], device_id=target, device_id_type=MESH,
            )
        )
    small.append(
        pltpu.make_async_remote_copy(
            src_ref=step_own, dst_ref=both_steps.at[core], send_sem=small_send.at[3],
            recv_sem=small_recv.at[3], device_id=partner, device_id_type=MESH,
        )
    )
    for copy in small:
        copy.start()
    outward = [
        pltpu.make_async_copy(src, dst, local.at[k])
        for k, (src, dst) in enumerate(
            (
                (proj_own, all_proj.at[me]),
                (tables_own, all_tables.at[me]),
                (rates_own, all_rates.at[me]),
                (step_own, both_steps.at[core]),
            )
        )
    ]
    for copy in outward:
        copy.start()

    arrivals = (
        (left, 0, 0, to_right, 4),
        (right, 1, 2, to_left, 5),
        (left, 1, 1, None, None),
        (right, 0, 3, None, None),
        (across, 0, 4, None, None),
        (across, 1, 5, None, None),
    )
    for shard, quarter, slot, onward, onward_slot in arrivals:
        for k in (1, 0):
            piece(k, shard, quarter, k * 12 + slot, partner).wait_recv()
            if onward is not None:
                go(piece(k, shard, quarter, k * 12 + onward_slot, onward))
            go(piece(k, shard, quarter, k * 12 + 6 + slot, partner))

    def partner_rows(k, quarter):
        quarter_rows = pairs[k][0].shape[0] // 4
        return pl.ds(
            pl.multiple_of(((1 - core) * 2 + quarter) * quarter_rows, quarter_rows), quarter_rows
        )

    for shard, quarter, slot, _, _ in arrivals:
        for k in (1, 0):
            dst = pairs[k][1].at[shard, partner_rows(k, quarter)]
            remote(dst, dst, k * 12 + 6 + slot, partner).wait_recv()
    for copy in small:
        copy.wait_recv()
    for copy in started + small:
        copy.wait_send()
    for copy in outward:
        copy.wait()


def gather_over_tp(proj, tables, rates, step):
    count = lax.axis_size("tp")
    spec = pl.BlockSpec(memory_space=pl.ANY)
    return pl.pallas_call(
        gather_kernel,
        out_shape=(
            jax.ShapeDtypeStruct((count, *proj.shape), proj.dtype),
            jax.ShapeDtypeStruct((count, *tables.shape), tables.dtype),
            jax.ShapeDtypeStruct((count, *rates.shape), rates.dtype),
            jax.ShapeDtypeStruct((2, *step.shape), step.dtype),
        ),
        in_specs=[spec] * 4,
        out_specs=(spec,) * 4,
        scratch_shapes=[
            pltpu.VMEM(proj.shape, proj.dtype),
            pltpu.VMEM(tables.shape, tables.dtype),
            pltpu.VMEM(rates.shape, rates.dtype),
            pltpu.VMEM(step.shape, step.dtype),
            pltpu.SemaphoreType.DMA((24,)),
            pltpu.SemaphoreType.DMA((24,)),
            pltpu.SemaphoreType.DMA((4,)),
            pltpu.SemaphoreType.DMA((4,)),
            pltpu.SemaphoreType.DMA((4,)),
        ],
        compiler_params=pltpu.CompilerParams(
            collective_id=0, has_side_effects=True, vmem_limit_bytes=4 << 20
        ),
        name="gather_over_tp",
    )(proj, tables, rates, step)


def mixer_kernel(
    tokens, proj, tables, rates, steps, in_gain, out_gain, shaped,
    tok, wide, normed, drive, e_re, e_im, g_re, g_im, inj, pushed, total, answer, tau,
    send1, got1, carry_in, decays, plane_end, plane_got, plane_time, time_got, send3, got3,
    load, s1, r1, s2, r2, st, rt, s3, r3,
):
    rows = tok.shape[0]
    tp_count, sp_count = lax.axis_size("tp"), lax.axis_size("sp")
    planes = sp_count // 2
    members = 2 * tp_count
    me, sp = lax.axis_index("tp"), lax.axis_index("sp")
    core, plane = lax.rem(sp, 2), sp // 2
    place = core * tp_count + me
    tiles = e_re.shape[0]
    per_shard = tiles // tp_count
    shards = tp_count

    def member(k):
        return {"sp": plane * 2 + k // tp_count, "tp": k % tp_count}

    def at_plane(z):
        return {"sp": z * 2 + core}

    barrier = pltpu.get_barrier_semaphore()

    def greet(offset, carry):
        other = lax.rem(plane + offset, planes)
        pl.semaphore_signal(barrier, inc=1, device_id=at_plane(other), device_id_type=MESH)
        return carry

    lax.fori_loop(1, planes, greet, 0)
    for k in range(members):
        @pl.when(place != k)
        def _():
            pl.semaphore_signal(barrier, inc=1, device_id=member(k), device_id_type=MESH)

    loads = [
        pltpu.make_async_copy(tokens, tok, load.at[0]),
        pltpu.make_async_copy(proj, wide, load.at[1]),
    ]
    for copy in loads:
        copy.start()

    row = lax.broadcasted_iota(jnp.int32, (rows, LANES), 0)
    lane = lax.broadcasted_iota(jnp.int32, (rows, LANES), 1)
    step_rows = rows // LANES
    column = jnp.zeros((rows, 1), F32)
    for k in range(step_rows):
        line = steps[core, pl.ds(me * step_rows + k, 1), :]
        column += jnp.sum(
            jnp.where(lane + k * LANES <= row, jnp.broadcast_to(line, (rows, LANES)), 0.0),
            axis=1, keepdims=True,
        )
    tau[...] = jnp.broadcast_to(column, (rows, LANES))
    whole_plane = jnp.sum(jnp.sum(steps[0] + steps[1], axis=1, keepdims=True), axis=0, keepdims=True)
    plane_time[...] = jnp.broadcast_to(whole_plane, plane_time.shape)

    first_row = lax.broadcasted_iota(jnp.int32, (CHUNK, LANES), 0) == 0

    def tables_of(i, carry):
        shard, inner = i // per_shard, lax.rem(i, per_shard)
        rate = rates[shard, pl.ds(inner, 1), :]
        high, low = turns_of(rates[shard, pl.ds(per_shard + inner, 1), :])
        before_re = jnp.ones((CHUNK, LANES), F32)
        before_im = jnp.zeros((CHUNK, LANES), F32)
        for c in range(0, rows, CHUNK):
            here = pl.ds(c, CHUNK)
            times = tau[here, :]
            cosine, sine = rotation(high, low, times)
            exponent = rate * times
            shrink, grow = jnp.exp(-exponent), jnp.exp(exponent)
            e_re[i, here, :] = shrink * cosine
            e_im[i, here, :] = shrink * sine
            q_re, q_im = grow * cosine, -(grow * sine)
            turned_re, turned_im = pltpu.roll(q_re, 1, 0), pltpu.roll(q_im, 1, 0)
            g_re[i, here, :] = jnp.where(first_row, before_re, turned_re) - q_re
            g_im[i, here, :] = jnp.where(first_row, before_im, turned_im) - q_im
            before_re, before_im = turned_re, turned_im
        return carry

    lax.fori_loop(0, tiles, tables_of, 0)

    loads[0].wait()
    strip = 16

    def norm(i, carry):
        here = pl.ds(pl.multiple_of(i * strip, strip), strip)
        value = tok[here, :].astype(F32)
        scale = lax.rsqrt(jnp.mean(value * value, axis=1, keepdims=True) + 1e-06)
        normed[here, :] = (value * scale * in_gain[...]).astype(BF16)
        return carry

    lax.fori_loop(0, rows // strip, norm, 0)
    loads[1].wait()
    for t in range(0, shards, 2):
        both = jnp.dot(
            normed[...],
            jnp.concatenate([wide[t], wide[t + 1]], axis=1),
            preferred_element_type=F32,
        )
        drive[t] = both[:, :LANES].astype(BF16)
        drive[t + 1] = both[:, LANES:].astype(BF16)

    k_row = lax.broadcasted_iota(jnp.int32, (LANES, LANES), 0)
    k_lane = lax.broadcasted_iota(jnp.int32, (LANES, LANES), 1)
    group_rows = LANES // (2 * per_shard)

    def inject(i, half):
        shard, inner = i // per_shard, lax.rem(i, per_shard)
        mask = k_row // group_rows == 2 * inner + k_lane // CHUNK
        push = [
            jnp.where(mask, tables[shard, b * LANES : (b + 1) * LANES, :].astype(F32), 0.0).astype(BF16)
            for b in range(2)
        ]
        pushed[...] = jnp.dot(
            drive[shard], jnp.concatenate(push, axis=1), preferred_element_type=F32
        )
        sum_re = jnp.zeros((CHUNK, LANES), F32)
        sum_im = jnp.zeros((CHUNK, LANES), F32)
        for c in range(0, rows, CHUNK):
            here = pl.ds(c, CHUNK)
            u_re, u_im = pushed[here, :LANES], pushed[here, LANES:]
            a_re, a_im = g_re[i, here, :], g_im[i, here, :]
            w_re = a_re * u_re - a_im * u_im
            w_im = a_re * u_im + a_im * u_re
            sum_re += w_re
            sum_im += w_im
            inj[i, here, :LANES] = w_re.astype(BF16)
            inj[i, here, LANES:] = w_im.astype(BF16)
        t_re = jnp.sum(sum_re, axis=0, keepdims=True)
        t_im = jnp.sum(sum_im, axis=0, keepdims=True)
        d_re, d_im = e_re[i, rows - 1 : rows, :], e_im[i, rows - 1 : rows, :]
        part = i // 2
        send1[part, half : half + 1, :] = d_re * t_re - d_im * t_im
        send1[part, 2 + half : 3 + half, :] = d_re * t_im + d_im * t_re
        send1[part, 4 + half : 5 + half, :] = d_re
        send1[part, 6 + half : 7 + half, :] = d_im

    def inject_pair(part, carry):
        inject(2 * part, 0)
        inject(2 * part + 1, 1)
        return carry

    lax.fori_loop(0, tiles // 2, inject_pair, 0)

    pl.semaphore_wait(barrier, planes - 1 + members - 1)

    def copy1(k):
        return pltpu.make_async_remote_copy(
            src_ref=send1.at[k], dst_ref=got1.at[place], send_sem=s1.at[k], recv_sem=r1.at[place],
            device_id=member(k), device_id_type=MESH,
        )

    for k in range(members):
        @pl.when(place != k)
        def _():
            copy1(k).start()

    def copy_time(z):
        return pltpu.make_async_remote_copy(
            src_ref=plane_time, dst_ref=time_got.at[plane], send_sem=st.at[z],
            recv_sem=rt.at[plane], device_id=at_plane(z), device_id_type=MESH,
        )

    def loop(lower, upper, body):
        def step(z, carry):
            body(z)
            return carry

        lax.fori_loop(lower, upper, step, 0)

    loop(plane + 1, planes, lambda z: copy_time(z).start())
    got1[pl.ds(place, 1)] = send1[pl.ds(place, 1)]
    for k in range(members):
        @pl.when(place != k)
        def _():
            pltpu.make_async_remote_copy(
                src_ref=send1.at[k], dst_ref=got1.at[k], send_sem=s1.at[k], recv_sem=r1.at[k],
                device_id=member(k), device_id_type=MESH,
            ).wait_recv()

    def advance(k, re, im):
        block = got1[k]
        d_re, d_im = block[4:6], block[6:8]
        return d_re * re - d_im * im + block[0:2], d_re * im + d_im * re + block[2:4]

    nothing = jnp.zeros((2, LANES), F32)
    re, im = nothing, nothing
    for k in range(members):
        re, im = advance(k, re, im)
    plane_end[0:2, :] = re
    plane_end[2:4, :] = im

    def copy2(z):
        return pltpu.make_async_remote_copy(
            src_ref=plane_end, dst_ref=plane_got.at[plane], send_sem=s2.at[z],
            recv_sem=r2.at[plane], device_id=at_plane(z), device_id_type=MESH,
        )

    loop(plane + 1, planes, lambda z: copy2(z).start())

    p_row = lax.broadcasted_iota(jnp.int32, (rows, rows), 0)
    p_col = lax.broadcasted_iota(jnp.int32, (rows, rows), 1)
    lower = jnp.where(p_col <= p_row, 1.0, 0.0).astype(BF16)

    def prefix(i):
        total[i] = jnp.dot(lower, inj[i], preferred_element_type=F32)

    loop(0, tiles, prefix)

    def time_wait(z):
        pltpu.make_async_remote_copy(
            src_ref=plane_time, dst_ref=time_got.at[z], send_sem=st.at[z], recv_sem=rt.at[z],
            device_id=at_plane(z), device_id_type=MESH,
        ).wait_recv()

    loop(0, plane, time_wait)

    def plane_decay(z):
        times = jnp.broadcast_to(time_got[z], (1, LANES))
        for half in range(2):
            i = 2 * place + half
            shard, inner = i // per_shard, lax.rem(i, per_shard)
            rate = rates[shard, pl.ds(inner, 1), :]
            high, low = turns_of(rates[shard, pl.ds(per_shard + inner, 1), :])
            cosine, sine = rotation(high, low, times)
            shrink = jnp.exp(-(rate * times))
            decays[z, half : half + 1, :] = shrink * cosine
            decays[z, 2 + half : 3 + half, :] = shrink * sine

    loop(0, plane, plane_decay)

    def end_wait(z):
        pltpu.make_async_remote_copy(
            src_ref=plane_end, dst_ref=plane_got.at[z], send_sem=s2.at[z], recv_sem=r2.at[z],
            device_id=at_plane(z), device_id_type=MESH,
        ).wait_recv()

    loop(0, plane, end_wait)

    def earlier(z, carry):
        re, im = carry
        d, end = decays[z], plane_got[z]
        return (
            d[0:2] * re - d[2:4] * im + end[0:2],
            d[0:2] * im + d[2:4] * re + end[2:4],
        )

    re, im = lax.fori_loop(0, plane, earlier, (nothing, nothing))
    for k in range(members):
        send3[k, 0:2, :] = re
        send3[k, 2:4, :] = im
        if k < members - 1:
            re, im = advance(k, re, im)

    def copy3(k):
        return pltpu.make_async_remote_copy(
            src_ref=send3.at[k], dst_ref=got3.at[place], send_sem=s3.at[k], recv_sem=r3.at[place],
            device_id=member(k), device_id_type=MESH,
        )

    for k in range(members):
        @pl.when(place != k)
        def _():
            copy3(k).start()
    got3[pl.ds(place, 1)] = send3[pl.ds(place, 1)]
    for k in range(members):
        @pl.when(place != k)
        def _():
            pltpu.make_async_remote_copy(
                src_ref=send3.at[k], dst_ref=got3.at[k], send_sem=s3.at[k], recv_sem=r3.at[k],
                device_id=member(k), device_id_type=MESH,
            ).wait_recv()

    answer[...] = jnp.zeros_like(answer)

    def respond(i, half):
        shard, inner = i // per_shard, lax.rem(i, per_shard)
        part = i // 2
        in_re = got3[part, half : half + 1, :]
        in_im = got3[part, 2 + half : 3 + half, :]
        for c in range(0, rows, CHUNK):
            here = pl.ds(c, CHUNK)
            a_re, a_im = total[i, here, :LANES] + in_re, total[i, here, LANES:] + in_im
            p_re, p_im = e_re[i, here, :], e_im[i, here, :]
            inj[i, here, :LANES] = (p_re * a_re - p_im * a_im).astype(BF16)
            inj[i, here, LANES:] = (p_re * a_im + p_im * a_re).astype(BF16)
        read = tables[shard, 2 * LANES :, :].astype(F32)
        lane_group = lax.broadcasted_iota(jnp.int32, (CHUNK, LANES), 1) // group_rows
        blocks = [
            jnp.where(lane_group == 2 * inner + g, read[b * CHUNK : (b + 1) * CHUNK], 0.0)
            for b in range(2)
            for g in range(2)
        ]
        answer[shard] += jnp.dot(
            inj[i], jnp.concatenate(blocks, axis=0).astype(BF16), preferred_element_type=F32
        )

    def respond_pair(part):
        respond(2 * part, 0)
        respond(2 * part + 1, 1)

    loop(0, tiles // 2, respond_pair)

    def finish(i):
        here = pl.ds(pl.multiple_of(i * CHUNK, CHUNK), CHUNK)
        values = []
        squares = jnp.zeros((CHUNK, LANES), F32)
        for t in range(shards):
            v = answer[t, here, :]
            v = 0.5 * v * (1.0 + jnp.tanh(0.7978845608 * (v + 0.044715 * (v * v * v))))
            v = v.astype(BF16).astype(F32)
            values.append(v)
            squares += v * v
        mean = jnp.sum(squares, axis=1, keepdims=True) * np.float32(1.0 / (shards * LANES))
        scale = lax.rsqrt(mean + 1e-06)
        for t in range(shards):
            line = pl.ds(t * LANES, LANES)
            shaped[here, line] = (values[t] * scale * out_gain[:, line]).astype(BF16)

    loop(0, rows // CHUNK, finish)

    for k in range(members):
        @pl.when(place != k)
        def _():
            copy1(k).wait_send()
            copy3(k).wait_send()
    loop(plane + 1, planes, lambda z: copy_time(z).wait_send())
    loop(plane + 1, planes, lambda z: copy2(z).wait_send())


def mix(tokens, proj, tables, rates, steps, in_gain, out_gain):
    rows, width = tokens.shape
    shards = lax.axis_size("tp")
    planes = lax.axis_size("sp") // 2
    members = 2 * shards
    tiles = shards * rates.shape[1] // 2
    vmem = pl.BlockSpec(memory_space=pltpu.VMEM)
    far = pl.BlockSpec(memory_space=pl.ANY)
    table = pltpu.VMEM((tiles, rows, LANES), F32)
    dma = pltpu.SemaphoreType.DMA
    return pl.pallas_call(
        mixer_kernel,
        out_shape=jax.ShapeDtypeStruct((rows, shards * LANES), BF16),
        in_specs=[far, far] + [vmem] * 5,
        out_specs=vmem,
        scratch_shapes=[
            pltpu.VMEM(tokens.shape, BF16),
            pltpu.VMEM(proj.shape, BF16),
            pltpu.VMEM(tokens.shape, BF16),
            pltpu.VMEM((shards, rows, LANES), BF16),
            table, table, table, table,
            pltpu.VMEM((tiles, rows, 2 * LANES), BF16),
            pltpu.VMEM((rows, 2 * LANES), F32),
            pltpu.VMEM((tiles, rows, 2 * LANES), F32),
            pltpu.VMEM((shards, rows, LANES), F32),
            pltpu.VMEM((rows, LANES), F32),
            pltpu.VMEM((members, 8, LANES), F32),
            pltpu.VMEM((members, 8, LANES), F32),
            pltpu.VMEM((4, LANES), F32),
            pltpu.VMEM((planes, 4, LANES), F32),
            pltpu.VMEM((4, LANES), F32),
            pltpu.VMEM((planes, 4, LANES), F32),
            pltpu.VMEM((1, LANES), F32),
            pltpu.VMEM((planes, 1, LANES), F32),
            pltpu.VMEM((members, 4, LANES), F32),
            pltpu.VMEM((members, 4, LANES), F32),
            dma((2,)),
            dma((members,)), dma((members,)),
            dma((planes,)), dma((planes,)),
            dma((planes,)), dma((planes,)),
            dma((members,)), dma((members,)),
        ],
        compiler_params=pltpu.CompilerParams(
            collective_id=1, has_side_effects=True, vmem_limit_bytes=48 << 20
        ),
        name="mixer",
    )(tokens, proj, tables, rates, steps, in_gain, out_gain)


def on_device(
    tokens, step, in_gain, in_proj, decay_rate, frequency, input_map, readout, out_gain, out_proj
):
    groups, states = decay_rate.shape
    lam_re, lam_im = -decay_rate[:, :, None], frequency[:, :, None]
    size = lam_re * lam_re + lam_im * lam_im
    b_re = (input_map[0] * lam_re + input_map[1] * lam_im) / size
    b_im = (input_map[1] * lam_re - input_map[0] * lam_im) / size
    rows = groups * input_map.shape[-1]
    push = jnp.stack([b_re, b_re, b_im, b_im]).transpose(1, 3, 0, 2).reshape(rows, 2, 2 * states)
    push = push.transpose(1, 0, 2).reshape(2 * rows, 2 * states)
    read = jnp.stack([readout[0], -readout[1]]).transpose(0, 3, 1, 2).reshape(2 * states, rows)
    tables = jnp.concatenate([push, read], axis=0).astype(BF16)
    rates = jnp.concatenate([decay_rate, frequency], axis=0).reshape(-1, LANES)
    proj, tables, rates, steps = gather_over_tp(in_proj, tables, rates, step.reshape(-1, LANES))
    shaped = mix(
        tokens, proj, tables, rates, steps, in_gain.reshape(1, -1), out_gain.reshape(1, -1)
    )
    return jnp.dot(shaped, out_proj, preferred_element_type=F32).astype(BF16)


def solution(mesh):
    placed = (
        P(("grp", "sp", "tp"), None),
        P(("grp", "sp")),
        P(),
        P(None, "tp"),
        P("tp", None),
        P("tp", None),
        P(None, "tp", None, None),
        P(None, "tp", None, None),
        P(),
        P(),
    )
    return jax.shard_map(
        on_device,
        mesh=mesh,
        in_specs=placed,
        out_specs=P(("grp", "sp", "tp"), None),
        check_vma=False,
    )
```

```python
import functools

import jax
import jax.numpy as jnp
import numpy as np
from jax import lax
from jax.experimental import pallas as pl
from jax.experimental.pallas import tpu as pltpu
from jax.sharding import PartitionSpec as P

F32, BF16 = jnp.float32, jnp.bfloat16
MESH = pl.DeviceIdType.MESH
LANES = 128
CHUNK = 64
SIN = (6.283182782944718, -41.34141729070845, 81.59606953187966, -76.57887013158442, 41.19977042473147, -12.262090350994187)
COS = (0.9999999888727491, -19.7392044313539, 64.939113609812, -85.45006239525888, 60.16694808625918, -25.96486025322117, 6.5245930831162795)
TURN = np.float32(1.0 / (2.0 * np.pi))
TURN_LOW = np.float32(1.0 / (2.0 * np.pi) - float(TURN))


def halves(value):
    wide = value * np.float32(4097.0)
    high = wide - (wide - value)
    return high, value - high


def turns_of(freqs):
    high = freqs * TURN
    f_high, f_low = halves(freqs)
    c_high, c_low = (np.float32(v) for v in halves(TURN))
    error = ((f_high * c_high - high) + f_high * c_low + f_low * c_high) + f_low * c_low
    return high, error + freqs * TURN_LOW


def polynomial(x, terms):
    total = jnp.full_like(x, np.float32(terms[-1]))
    for term in terms[-2::-1]:
        total = total * x + np.float32(term)
    return total


def rotation(high, low, times):
    whole = high * times
    part = (whole - jnp.round(whole)) + low * times
    square = part * part
    return polynomial(square, COS), polynomial(square, SIN) * part


def gather_over_tp(wide, tables, rates, proj_sent, proj_got, table_sent, table_got, rate_sent, rate_got):
    count, me = lax.axis_size("tp"), lax.axis_index("tp")
    right, left, across = (lax.rem(me + k, count) for k in (1, count - 1, 2))

    def piece(k, shard, half, slot, target):
        ref, sent, got = ((wide, proj_sent, proj_got), (tables, table_sent, table_got))[k]
        size = ref.shape[1] // 2
        where = ref.at[shard, pl.ds(half * size, size)]
        return pltpu.make_async_remote_copy(
            src_ref=where, dst_ref=where, send_sem=sent.at[slot], recv_sem=got.at[slot],
            device_id={"tp": target}, device_id_type=MESH,
        )

    started = []

    def go(copy):
        copy.start()
        started.append(copy)

    small = [
        pltpu.make_async_remote_copy(
            src_ref=rates.at[me], dst_ref=rates.at[me], send_sem=rate_sent.at[slot],
            recv_sem=rate_got.at[slot], device_id={"tp": target}, device_id_type=MESH,
        )
        for slot, target in enumerate((right, left, across))
    ]
    for copy in small:
        go(copy)
    for order in range(2):
        for k in (1, 0):
            go(piece(k, me, order, order, right))
            go(piece(k, me, 1 - order, 2 + order, left))
    for shard, half, slot, onward, onward_slot in (
        (left, 0, 0, right, 4),
        (right, 1, 2, left, 5),
        (left, 1, 1, None, None),
        (right, 0, 3, None, None),
        (across, 0, 4, None, None),
        (across, 1, 5, None, None),
    ):
        for k in (1, 0):
            piece(k, shard, half, slot, left).wait_recv()
            if onward is not None:
                go(piece(k, shard, half, onward_slot, onward))
    for copy in small:
        copy.wait_recv()
    for copy in started:
        copy.wait_send()


def own_tables(tables, rates, me, decay, frequency, input_map, readout):
    groups, states = decay.shape
    channels = input_map.shape[-1]
    pairs = groups // 2
    for g in range(groups):
        lanes = slice((g % 2) * states, (g % 2 + 1) * states)
        rates[me, g // 2 : g // 2 + 1, lanes] = decay[g : g + 1, :]
        rates[me, pairs + g // 2 : pairs + g // 2 + 1, lanes] = frequency[g : g + 1, :]

    def turned(value):
        size = value.shape[1]
        unit = jnp.where(
            lax.broadcasted_iota(jnp.int32, (size, size), 0)
            == lax.broadcasted_iota(jnp.int32, (size, size), 1),
            1.0, 0.0,
        ).astype(F32)
        return lax.dot_general(
            unit, value, (((1,), (1,)), ((), ())),
            precision=lax.Precision.HIGHEST, preferred_element_type=F32,
        )

    maps = [turned(input_map[c].reshape(groups * states, channels)) for c in range(2)]
    for k in range(pairs):
        lam_re = -rates[me, k : k + 1, :]
        lam_im = rates[me, pairs + k : pairs + k + 1, :]
        size = lam_re * lam_re + lam_im * lam_im
        m_re, m_im = (m[:, k * LANES : (k + 1) * LANES] for m in maps)
        at = 2 * channels * k
        tables[me, at : at + channels, :] = ((m_re * lam_re + m_im * lam_im) / size).astype(BF16)
        tables[me, at + channels : at + 2 * channels, :] = (
            (m_im * lam_re - m_re * lam_im) / size
        ).astype(BF16)
    for c, sign in ((0, 1.0), (1, -1.0)):
        value = sign * turned(readout[c].reshape(groups * channels, states))
        tables[me, LANES + c * states : LANES + (c + 1) * states, :] = value.astype(BF16)


def mixer_kernel(
    tokens, proj, decay, frequency, input_map, readout, step, in_gain, out_gain, shaped,
    tok, wide, tables, rates, steps, decay_in, frequency_in, input_map_in, readout_in,
    normed, drive, e_re, e_im, g_re, g_im, inj, pushed, total, answer, tau,
    send1, got1, decays, plane_end, plane_got, plane_time, time_got, send3, got3,
    load, s1, r1, s2, r2, st, rt, s3, r3,
    proj_sent, proj_got, table_sent, table_got, rate_sent, rate_got, pass_sent, pass_got,
    ready, all_in,
):
    rows = tok.shape[0]
    tp_count, sp_count = lax.axis_size("tp"), lax.axis_size("sp")
    planes = sp_count // 2
    members = 2 * tp_count
    me, sp = lax.axis_index("tp"), lax.axis_index("sp")
    core, plane = lax.rem(sp, 2), sp // 2
    place = core * tp_count + me
    tiles = e_re.shape[0]
    per_shard = tiles // tp_count
    shards = tp_count

    def member(k):
        return {"sp": plane * 2 + k // tp_count, "tp": k % tp_count}

    def at_plane(z):
        return {"sp": z * 2 + core}

    partner = {"sp": sp + 1 - 2 * core}
    leads = place == 0

    def loop(lower, upper, body):
        def step(z, carry):
            body(z)
            return carry

        lax.fori_loop(lower, upper, step, 0)

    barrier = pltpu.get_barrier_semaphore()

    def greet(target):
        pl.semaphore_signal(barrier, inc=1, device_id=target, device_id_type=MESH)

    loop(0, plane, lambda z: greet({"sp": 2 * z}))

    @pl.when(core == 1)
    def _():
        for k in range(1, tp_count):
            greet({"tp": lax.rem(me + k, tp_count)})
        greet(partner)

    @pl.when(jnp.logical_and(jnp.logical_not(leads), place != tp_count))
    def _():
        greet({"sp": 2 * plane, "tp": 0})

    loads = [
        pltpu.make_async_copy(tokens, tok, load.at[0]),
        pltpu.make_async_copy(proj, wide.at[me], load.at[1]),
    ]
    for copy in loads:
        copy.start()

    passed = [
        (rates, rates),
        (tables, tables),
        *((wide.at[lax.rem(me + k, tp_count)],) * 2 for k in range(1, tp_count)),
        (step, steps.at[1]),
    ]

    def pass_on(slot):
        src, dst = passed[slot]
        return pltpu.make_async_remote_copy(
            src_ref=src, dst_ref=dst, send_sem=pass_sent.at[slot], recv_sem=pass_got.at[slot],
            device_id=partner, device_id_type=MESH,
        )

    def pass_back():
        slot = len(passed)
        return pltpu.make_async_remote_copy(
            src_ref=step, dst_ref=steps.at[0], send_sem=pass_sent.at[slot],
            recv_sem=pass_got.at[slot], device_id=partner, device_id_type=MESH,
        )

    @pl.when(core == 1)
    def _():
        inward = [
            pltpu.make_async_copy(src, dst, load.at[2 + k])
            for k, (src, dst) in enumerate(
                (
                    (decay, decay_in),
                    (frequency, frequency_in),
                    (input_map, input_map_in),
                    (readout, readout_in),
                )
            )
        ]
        for copy in inward:
            copy.start()
        for copy in inward:
            copy.wait()
        own_tables(tables, rates, me, decay_in, frequency_in, input_map_in, readout_in)
        loads[1].wait()
        pl.semaphore_wait(barrier, tp_count - 1)
        gather_over_tp(
            wide, tables, rates, proj_sent, proj_got, table_sent, table_got, rate_sent, rate_got
        )

    later = 2 * (planes - 1 - plane)

    @pl.when(leads)
    def _():
        pl.semaphore_wait(barrier, members - 1 + later)
        pl.semaphore_signal(ready, inc=1, device_id=partner, device_id_type=MESH)
        for k in range(1, members):
            pl.semaphore_signal(all_in, inc=1, device_id=member(k), device_id_type=MESH)

    @pl.when(jnp.logical_and(core == 0, jnp.logical_not(leads)))
    def _():
        pl.semaphore_wait(barrier, 1 + later)
        pl.semaphore_signal(ready, inc=1, device_id=partner, device_id_type=MESH)

    @pl.when(core == 0)
    def _():
        pass_back().start()

    row = lax.broadcasted_iota(jnp.int32, (rows, LANES), 0)
    lane = lax.broadcasted_iota(jnp.int32, (rows, LANES), 1)
    step_rows = rows // LANES
    column = jnp.zeros((rows, 1), F32)
    for k in range(step_rows):
        line = step[pl.ds(me * step_rows + k, 1), :]
        column += jnp.sum(
            jnp.where(lane + k * LANES <= row, jnp.broadcast_to(line, (rows, LANES)), 0.0),
            axis=1, keepdims=True,
        )
    tau[...] = jnp.broadcast_to(column, (rows, LANES))
    loads[0].wait()
    strip = 16

    def norm(i, carry):
        here = pl.ds(pl.multiple_of(i * strip, strip), strip)
        value = tok[here, :].astype(F32)
        scale = lax.rsqrt(jnp.mean(value * value, axis=1, keepdims=True) + 1e-06)
        normed[here, :] = (value * scale * in_gain[...]).astype(BF16)
        return carry

    lax.fori_loop(0, rows // strip, norm, 0)
    @pl.when(core == 0)
    def _():
        pass_on(0).wait_recv()

    first_row = lax.broadcasted_iota(jnp.int32, (CHUNK, LANES), 0) == 0

    def tables_of(i, carry):
        shard, inner = i // per_shard, lax.rem(i, per_shard)
        rate = rates[shard, pl.ds(inner, 1), :]
        high, low = turns_of(rates[shard, pl.ds(per_shard + inner, 1), :])
        before_re = jnp.ones((CHUNK, LANES), F32)
        before_im = jnp.zeros((CHUNK, LANES), F32)
        for c in range(0, rows, CHUNK):
            here = pl.ds(c, CHUNK)
            times = tau[here, :]
            cosine, sine = rotation(high, low, times)
            exponent = rate * times
            shrink, grow = jnp.exp(-exponent), jnp.exp(exponent)
            e_re[i, here, :] = shrink * cosine
            e_im[i, here, :] = shrink * sine
            q_re, q_im = grow * cosine, -(grow * sine)
            turned_re, turned_im = pltpu.roll(q_re, 1, 0), pltpu.roll(q_im, 1, 0)
            g_re[i, here, :] = jnp.where(first_row, before_re, turned_re) - q_re
            g_im[i, here, :] = jnp.where(first_row, before_im, turned_im) - q_im
            before_re, before_im = turned_re, turned_im
        return carry

    lax.fori_loop(0, tiles, tables_of, 0)

    @pl.when(core == 0)
    def _():
        loads[1].wait()
        for slot in range(1, len(passed)):
            pass_on(slot).wait_recv()

    for t in range(0, shards, 2):
        both = jnp.dot(
            normed[...],
            jnp.concatenate([wide[t], wide[t + 1]], axis=1),
            preferred_element_type=F32,
        )
        drive[t] = both[:, :LANES].astype(BF16)
        drive[t + 1] = both[:, LANES:].astype(BF16)

    k_row = lax.broadcasted_iota(jnp.int32, (LANES, LANES), 0)
    k_lane = lax.broadcasted_iota(jnp.int32, (LANES, LANES), 1)
    group_rows = LANES // (2 * per_shard)

    def inject(i, half):
        shard, inner = i // per_shard, lax.rem(i, per_shard)
        mask = k_row // group_rows == 2 * inner + k_lane // CHUNK
        push = [
            jnp.where(
                mask,
                jnp.concatenate(
                    [
                        tables[
                            shard,
                            pl.ds(pl.multiple_of((2 * inner + b) * group_rows, group_rows), group_rows),
                            :,
                        ].astype(F32)
                    ]
                    * (LANES // group_rows),
                    axis=0,
                ),
                0.0,
            ).astype(BF16)
            for b in range(2)
        ]
        pushed[...] = jnp.dot(
            drive[shard], jnp.concatenate(push, axis=1), preferred_element_type=F32
        )
        sum_re = jnp.zeros((CHUNK, LANES), F32)
        sum_im = jnp.zeros((CHUNK, LANES), F32)
        for c in range(0, rows, CHUNK):
            here = pl.ds(c, CHUNK)
            u_re, u_im = pushed[here, :LANES], pushed[here, LANES:]
            a_re, a_im = g_re[i, here, :], g_im[i, here, :]
            w_re = a_re * u_re - a_im * u_im
            w_im = a_re * u_im + a_im * u_re
            sum_re += w_re
            sum_im += w_im
            inj[i, here, :LANES] = w_re.astype(BF16)
            inj[i, here, LANES:] = w_im.astype(BF16)
        t_re = jnp.sum(sum_re, axis=0, keepdims=True)
        t_im = jnp.sum(sum_im, axis=0, keepdims=True)
        d_re, d_im = e_re[i, rows - 1 : rows, :], e_im[i, rows - 1 : rows, :]
        part = i // 2
        send1[part, half : half + 1, :] = d_re * t_re - d_im * t_im
        send1[part, 2 + half : 3 + half, :] = d_re * t_im + d_im * t_re
        send1[part, 4 + half : 5 + half, :] = d_re
        send1[part, 6 + half : 7 + half, :] = d_im

    def inject_pair(part, carry):
        inject(2 * part, 0)
        inject(2 * part + 1, 1)
        return carry

    lax.fori_loop(0, tiles // 2, inject_pair, 0)

    @pl.when(core == 1)
    def _():
        pl.semaphore_wait(ready, 1)
        for slot in range(len(passed)):
            pass_on(slot).start()

    @pl.when(jnp.logical_not(leads))
    def _():
        pl.semaphore_wait(all_in, 1)

    def copy1(k):
        return pltpu.make_async_remote_copy(
            src_ref=send1.at[k], dst_ref=got1.at[place], send_sem=s1.at[k], recv_sem=r1.at[place],
            device_id=member(k), device_id_type=MESH,
        )

    for k in range(members):
        @pl.when(place != k)
        def _():
            copy1(k).start()

    def copy_time(z):
        return pltpu.make_async_remote_copy(
            src_ref=plane_time, dst_ref=time_got.at[plane], send_sem=st.at[z],
            recv_sem=rt.at[plane], device_id=at_plane(z), device_id_type=MESH,
        )

    @pl.when(core == 1)
    def _():
        pass_back().wait_recv()

    steps[pl.ds(core, 1)] = step[...].reshape(1, *step.shape)
    whole_plane = jnp.sum(jnp.sum(steps[0] + steps[1], axis=1, keepdims=True), axis=0, keepdims=True)
    plane_time[...] = jnp.broadcast_to(whole_plane, plane_time.shape)
    loop(plane + 1, planes, lambda z: copy_time(z).start())
    got1[pl.ds(place, 1)] = send1[pl.ds(place, 1)]
    for k in range(members):
        @pl.when(place != k)
        def _():
            pltpu.make_async_remote_copy(
                src_ref=send1.at[k], dst_ref=got1.at[k], send_sem=s1.at[k], recv_sem=r1.at[k],
                device_id=member(k), device_id_type=MESH,
            ).wait_recv()

    def advance(k, re, im):
        block = got1[k]
        d_re, d_im = block[4:6], block[6:8]
        return d_re * re - d_im * im + block[0:2], d_re * im + d_im * re + block[2:4]

    nothing = jnp.zeros((2, LANES), F32)
    re, im = nothing, nothing
    for k in range(members):
        re, im = advance(k, re, im)
    plane_end[0:2, :] = re
    plane_end[2:4, :] = im

    def copy2(z):
        return pltpu.make_async_remote_copy(
            src_ref=plane_end, dst_ref=plane_got.at[plane], send_sem=s2.at[z],
            recv_sem=r2.at[plane], device_id=at_plane(z), device_id_type=MESH,
        )

    loop(plane + 1, planes, lambda z: copy2(z).start())

    p_row = lax.broadcasted_iota(jnp.int32, (rows, rows), 0)
    p_col = lax.broadcasted_iota(jnp.int32, (rows, rows), 1)
    lower = jnp.where(p_col <= p_row, 1.0, 0.0).astype(BF16)

    def prefix(i):
        total[i] = jnp.dot(lower, inj[i], preferred_element_type=F32)

    loop(0, tiles, prefix)

    def time_wait(z):
        pltpu.make_async_remote_copy(
            src_ref=plane_time, dst_ref=time_got.at[z], send_sem=st.at[z], recv_sem=rt.at[z],
            device_id=at_plane(z), device_id_type=MESH,
        ).wait_recv()

    loop(0, plane, time_wait)

    def plane_decay(z):
        times = jnp.broadcast_to(time_got[z], (1, LANES))
        for half in range(2):
            i = 2 * place + half
            shard, inner = i // per_shard, lax.rem(i, per_shard)
            rate = rates[shard, pl.ds(inner, 1), :]
            high, low = turns_of(rates[shard, pl.ds(per_shard + inner, 1), :])
            cosine, sine = rotation(high, low, times)
            shrink = jnp.exp(-(rate * times))
            decays[z, half : half + 1, :] = shrink * cosine
            decays[z, 2 + half : 3 + half, :] = shrink * sine

    loop(0, plane, plane_decay)

    def end_wait(z):
        pltpu.make_async_remote_copy(
            src_ref=plane_end, dst_ref=plane_got.at[z], send_sem=s2.at[z], recv_sem=r2.at[z],
            device_id=at_plane(z), device_id_type=MESH,
        ).wait_recv()

    loop(0, plane, end_wait)

    def earlier(z, carry):
        re, im = carry
        d, end = decays[z], plane_got[z]
        return (
            d[0:2] * re - d[2:4] * im + end[0:2],
            d[0:2] * im + d[2:4] * re + end[2:4],
        )

    re, im = lax.fori_loop(0, plane, earlier, (nothing, nothing))
    for k in range(members):
        send3[k, 0:2, :] = re
        send3[k, 2:4, :] = im
        if k < members - 1:
            re, im = advance(k, re, im)

    def copy3(k):
        return pltpu.make_async_remote_copy(
            src_ref=send3.at[k], dst_ref=got3.at[place], send_sem=s3.at[k], recv_sem=r3.at[place],
            device_id=member(k), device_id_type=MESH,
        )

    for k in range(members):
        @pl.when(place != k)
        def _():
            copy3(k).start()
    got3[pl.ds(place, 1)] = send3[pl.ds(place, 1)]
    for k in range(members):
        @pl.when(place != k)
        def _():
            pltpu.make_async_remote_copy(
                src_ref=send3.at[k], dst_ref=got3.at[k], send_sem=s3.at[k], recv_sem=r3.at[k],
                device_id=member(k), device_id_type=MESH,
            ).wait_recv()

    answer[...] = jnp.zeros_like(answer)

    def respond(i, half):
        shard, inner = i // per_shard, lax.rem(i, per_shard)
        part = i // 2
        in_re = got3[part, half : half + 1, :]
        in_im = got3[part, 2 + half : 3 + half, :]
        for c in range(0, rows, CHUNK):
            here = pl.ds(c, CHUNK)
            a_re, a_im = total[i, here, :LANES] + in_re, total[i, here, LANES:] + in_im
            p_re, p_im = e_re[i, here, :], e_im[i, here, :]
            inj[i, here, :LANES] = (p_re * a_re - p_im * a_im).astype(BF16)
            inj[i, here, LANES:] = (p_re * a_im + p_im * a_re).astype(BF16)
        read = tables[shard, LANES:, :].astype(F32)
        lane_group = lax.broadcasted_iota(jnp.int32, (CHUNK, LANES), 1) // group_rows
        blocks = [
            jnp.where(lane_group == 2 * inner + g, read[b * CHUNK : (b + 1) * CHUNK], 0.0)
            for b in range(2)
            for g in range(2)
        ]
        answer[shard] += jnp.dot(
            inj[i], jnp.concatenate(blocks, axis=0).astype(BF16), preferred_element_type=F32
        )

    def respond_pair(part):
        respond(2 * part, 0)
        respond(2 * part + 1, 1)

    loop(0, tiles // 2, respond_pair)

    def finish(i):
        here = pl.ds(pl.multiple_of(i * CHUNK, CHUNK), CHUNK)
        values = []
        squares = jnp.zeros((CHUNK, LANES), F32)
        for t in range(shards):
            v = answer[t, here, :]
            v = 0.5 * v * (1.0 + jnp.tanh(0.7978845608 * (v + 0.044715 * (v * v * v))))
            v = v.astype(BF16).astype(F32)
            values.append(v)
            squares += v * v
        mean = jnp.sum(squares, axis=1, keepdims=True) * np.float32(1.0 / (shards * LANES))
        scale = lax.rsqrt(mean + 1e-06)
        for t in range(shards):
            line = pl.ds(t * LANES, LANES)
            shaped[here, line] = (values[t] * scale * out_gain[:, line]).astype(BF16)

    loop(0, rows // CHUNK, finish)

    for k in range(members):
        @pl.when(place != k)
        def _():
            copy1(k).wait_send()
            copy3(k).wait_send()
    loop(plane + 1, planes, lambda z: copy_time(z).wait_send())
    loop(plane + 1, planes, lambda z: copy2(z).wait_send())

    @pl.when(core == 1)
    def _():
        for slot in range(len(passed)):
            pass_on(slot).wait_send()

    @pl.when(core == 0)
    def _():
        pass_back().wait_send()


def mix(tokens, proj, decay, frequency, input_map, readout, step, in_gain, out_gain):
    rows, width = tokens.shape
    shards = lax.axis_size("tp")
    planes = lax.axis_size("sp") // 2
    members = 2 * shards
    pairs = decay.size // LANES
    tiles = shards * pairs
    vmem = pl.BlockSpec(memory_space=pltpu.VMEM)
    far = pl.BlockSpec(memory_space=pl.ANY)
    table = pltpu.VMEM((tiles, rows, LANES), F32)
    dma = pltpu.SemaphoreType.DMA
    passed = shards + 3
    return pl.pallas_call(
        mixer_kernel,
        out_shape=jax.ShapeDtypeStruct((rows, shards * LANES), BF16),
        in_specs=[far] * 6 + [vmem] * 3,
        out_specs=vmem,
        scratch_shapes=[
            pltpu.VMEM(tokens.shape, BF16),
            pltpu.VMEM((shards, *proj.shape), BF16),
            pltpu.VMEM((shards, 2 * LANES, LANES), BF16),
            pltpu.VMEM((shards, 2 * pairs, LANES), F32),
            pltpu.VMEM((2, *step.shape), F32),
            *(pltpu.VMEM(a.shape, F32) for a in (decay, frequency, input_map, readout)),
            pltpu.VMEM(tokens.shape, BF16),
            pltpu.VMEM((shards, rows, LANES), BF16),
            table, table, table, table,
            pltpu.VMEM((tiles, rows, 2 * LANES), BF16),
            pltpu.VMEM((rows, 2 * LANES), F32),
            pltpu.VMEM((tiles, rows, 2 * LANES), F32),
            pltpu.VMEM((shards, rows, LANES), F32),
            pltpu.VMEM((rows, LANES), F32),
            pltpu.VMEM((members, 8, LANES), F32),
            pltpu.VMEM((members, 8, LANES), F32),
            pltpu.VMEM((planes, 4, LANES), F32),
            pltpu.VMEM((4, LANES), F32),
            pltpu.VMEM((planes, 4, LANES), F32),
            pltpu.VMEM((1, LANES), F32),
            pltpu.VMEM((planes, 1, LANES), F32),
            pltpu.VMEM((members, 4, LANES), F32),
            pltpu.VMEM((members, 4, LANES), F32),
            dma((6,)),
            dma((members,)), dma((members,)),
            dma((planes,)), dma((planes,)),
            dma((planes,)), dma((planes,)),
            dma((members,)), dma((members,)),
            dma((6,)), dma((6,)), dma((6,)), dma((6,)), dma((3,)), dma((3,)),
            dma((passed,)), dma((passed,)),
            pltpu.SemaphoreType.REGULAR,
            pltpu.SemaphoreType.REGULAR,
        ],
        compiler_params=pltpu.CompilerParams(
            collective_id=0, has_side_effects=True, vmem_limit_bytes=48 << 20
        ),
        name="mixer",
    )(tokens, proj, decay, frequency, input_map, readout, step, in_gain, out_gain)


def on_device(
    tokens, step, in_gain, in_proj, decay_rate, frequency, input_map, readout, out_gain, out_proj
):
    shaped = mix(
        tokens, in_proj, decay_rate, frequency, input_map, readout,
        step.reshape(-1, LANES), in_gain.reshape(1, -1), out_gain.reshape(1, -1),
    )
    return jnp.dot(shaped, out_proj, preferred_element_type=F32).astype(BF16)


def solution(mesh):
    placed = (
        P(("grp", "sp", "tp"), None),
        P(("grp", "sp")),
        P(),
        P(None, "tp"),
        P("tp", None),
        P("tp", None),
        P(None, "tp", None, None),
        P(None, "tp", None, None),
        P(),
        P(),
    )
    return jax.shard_map(
        on_device,
        mesh=mesh,
        in_specs=placed,
        out_specs=P(("grp", "sp", "tp"), None),
        check_vma=False,
    )
```

```python
import functools

import jax
import jax.numpy as jnp
import numpy as np
from jax import lax
from jax.experimental import pallas as pl
from jax.experimental.pallas import tpu as pltpu
from jax.sharding import PartitionSpec as P

F32, BF16 = jnp.float32, jnp.bfloat16
MESH = pl.DeviceIdType.MESH
LANES = 128
CHUNK = 64
SIN = (6.283182782944718, -41.34141729070845, 81.59606953187966, -76.57887013158442, 41.19977042473147, -12.262090350994187)
COS = (0.9999999888727491, -19.7392044313539, 64.939113609812, -85.45006239525888, 60.16694808625918, -25.96486025322117, 6.5245930831162795)
TURN = np.float32(1.0 / (2.0 * np.pi))
TURN_LOW = np.float32(1.0 / (2.0 * np.pi) - float(TURN))


def halves(value):
    wide = value * np.float32(4097.0)
    high = wide - (wide - value)
    return high, value - high


def turns_of(freqs):
    high = freqs * TURN
    f_high, f_low = halves(freqs)
    c_high, c_low = (np.float32(v) for v in halves(TURN))
    error = ((f_high * c_high - high) + f_high * c_low + f_low * c_high) + f_low * c_low
    return high, error + freqs * TURN_LOW


def polynomial(x, terms):
    total = jnp.full_like(x, np.float32(terms[-1]))
    for term in terms[-2::-1]:
        total = total * x + np.float32(term)
    return total


def rotation(high, low, times):
    whole = high * times
    part = (whole - jnp.round(whole)) + low * times
    square = part * part
    return polynomial(square, COS), polynomial(square, SIN) * part


def gather_over_tp(wide, tables, rates, proj_sent, proj_got, table_sent, table_got, rate_sent, rate_got):
    count, me = lax.axis_size("tp"), lax.axis_index("tp")
    right, left, across = (lax.rem(me + k, count) for k in (1, count - 1, 2))

    def piece(k, shard, half, slot, target):
        ref, sent, got = ((wide, proj_sent, proj_got), (tables, table_sent, table_got))[k]
        size = ref.shape[1] // 2
        where = ref.at[shard, pl.ds(half * size, size)]
        return pltpu.make_async_remote_copy(
            src_ref=where, dst_ref=where, send_sem=sent.at[slot], recv_sem=got.at[slot],
            device_id={"tp": target}, device_id_type=MESH,
        )

    started = []

    def go(copy):
        copy.start()
        started.append(copy)

    small = [
        pltpu.make_async_remote_copy(
            src_ref=rates.at[me], dst_ref=rates.at[me], send_sem=rate_sent.at[slot],
            recv_sem=rate_got.at[slot], device_id={"tp": target}, device_id_type=MESH,
        )
        for slot, target in enumerate((right, left, across))
    ]
    for copy in small:
        go(copy)
    for order in range(2):
        for k in (1, 0):
            go(piece(k, me, order, order, right))
            go(piece(k, me, 1 - order, 2 + order, left))
    for shard, half, slot, onward, onward_slot in (
        (left, 0, 0, right, 4),
        (right, 1, 2, left, 5),
        (left, 1, 1, None, None),
        (right, 0, 3, None, None),
        (across, 0, 4, None, None),
        (across, 1, 5, None, None),
    ):
        for k in (1, 0):
            piece(k, shard, half, slot, left).wait_recv()
            if onward is not None:
                go(piece(k, shard, half, onward_slot, onward))
    for copy in small:
        copy.wait_recv()
    for copy in started:
        copy.wait_send()


def own_tables(tables, rates, me, decay, frequency, input_map, readout, paired):
    groups, states = decay.shape
    channels = input_map.shape[-2]
    pairs = groups // 2
    for g in range(groups):
        lanes = slice((g % 2) * states, (g % 2 + 1) * states)
        rates[me, g // 2 : g // 2 + 1, lanes] = decay[g : g + 1, :]
        rates[me, pairs + g // 2 : pairs + g // 2 + 1, lanes] = frequency[g : g + 1, :]
        for c in range(2):
            paired[c, g // 2, :, lanes] = input_map[c, g]

    def turned(value):
        size = value.shape[1]
        unit = jnp.where(
            lax.broadcasted_iota(jnp.int32, (size, size), 0)
            == lax.broadcasted_iota(jnp.int32, (size, size), 1),
            1.0, 0.0,
        ).astype(F32)
        return lax.dot_general(
            unit, value, (((1,), (1,)), ((), ())),
            precision=lax.Precision.HIGHEST, preferred_element_type=F32,
        )

    for k in range(pairs):
        lam_re = -rates[me, k : k + 1, :]
        lam_im = rates[me, pairs + k : pairs + k + 1, :]
        size = lam_re * lam_re + lam_im * lam_im
        m_re, m_im = paired[0, k], paired[1, k]
        at = 2 * channels * k
        tables[me, at : at + channels, :] = ((m_re * lam_re + m_im * lam_im) / size).astype(BF16)
        tables[me, at + channels : at + 2 * channels, :] = (
            (m_im * lam_re - m_re * lam_im) / size
        ).astype(BF16)
    for c, sign in ((0, 1.0), (1, -1.0)):
        value = sign * turned(readout[c].reshape(groups * channels, states))
        tables[me, LANES + c * states : LANES + (c + 1) * states, :] = value.astype(BF16)


def mixer_kernel(
    tokens, proj, decay, frequency, input_map, readout, step_hbm, in_gain_hbm, out_gain_hbm, shaped,
    tok, wide, tables, rates, steps, step, in_gain, out_gain,
    decay_in, frequency_in, input_map_in, readout_in, paired,
    normed, drive, e_re, e_im, g_re, g_im, inj, pushed, total, answer, tau,
    send1, got1, decays, plane_end, plane_got, plane_time, time_got, send3, got3,
    load, s1, r1, s2, r2, st, rt, s3, r3,
    proj_sent, proj_got, table_sent, table_got, rate_sent, rate_got, pass_sent, pass_got,
    ready, all_in,
):
    rows = tok.shape[0]
    tp_count, sp_count = lax.axis_size("tp"), lax.axis_size("sp")
    planes = sp_count // 2
    members = 2 * tp_count
    me, sp = lax.axis_index("tp"), lax.axis_index("sp")
    core, plane = lax.rem(sp, 2), sp // 2
    place = core * tp_count + me
    tiles = e_re.shape[0]
    per_shard = tiles // tp_count
    shards = tp_count

    def member(k):
        return {"sp": plane * 2 + k // tp_count, "tp": k % tp_count}

    def at_plane(z):
        return {"sp": z * 2 + core}

    partner = {"sp": sp + 1 - 2 * core}

    def loop(lower, upper, body):
        def step(z, carry):
            body(z)
            return carry

        lax.fori_loop(lower, upper, step, 0)

    hub = 1
    first_chip = me == 0
    barrier = pltpu.get_barrier_semaphore()

    def greet(target):
        pl.semaphore_signal(barrier, inc=1, device_id=target, device_id_type=MESH)

    loads = [
        pltpu.make_async_copy(src, dst, load.at[k])
        for k, (src, dst) in enumerate(
            (
                (tokens, tok),
                (proj, wide.at[me]),
                (step_hbm, step),
                (in_gain_hbm, in_gain),
                (out_gain_hbm, out_gain),
            )
        )
    ]

    @pl.when(core == 1)
    def _():
        for k in range(1, tp_count):
            greet({"tp": lax.rem(me + k, tp_count)})

    @pl.when((core == 0) != first_chip)
    def _():
        greet(partner)

    @pl.when(place != hub)
    def _():
        greet(member(hub))

    for k in (2, 0, 1, 3, 4):
        loads[k].start()
    loop(0, plane, lambda z: greet({"sp": 2 * z, "tp": hub}))

    passed = [
        (rates, rates),
        (tables, tables),
        *((wide.at[lax.rem(me + k, tp_count)],) * 2 for k in range(1, tp_count)),
        (step, steps.at[1]),
    ]

    def pass_on(slot):
        src, dst = passed[slot]
        return pltpu.make_async_remote_copy(
            src_ref=src, dst_ref=dst, send_sem=pass_sent.at[slot], recv_sem=pass_got.at[slot],
            device_id=partner, device_id_type=MESH,
        )

    def pass_back():
        slot = len(passed)
        return pltpu.make_async_remote_copy(
            src_ref=step, dst_ref=steps.at[0], send_sem=pass_sent.at[slot],
            recv_sem=pass_got.at[slot], device_id=partner, device_id_type=MESH,
        )

    def pass_all():
        for slot in (0, *range(2, len(passed)), 1):
            pass_on(slot).start()

    @pl.when(core == 1)
    def _():
        inward = [
            pltpu.make_async_copy(src, dst, load.at[len(loads) + k])
            for k, (src, dst) in enumerate(
                (
                    (decay, decay_in),
                    (frequency, frequency_in),
                    (input_map, input_map_in),
                    (readout, readout_in),
                )
            )
        ]
        for copy in inward:
            copy.start()
        for copy in inward:
            copy.wait()
        own_tables(
            tables, rates, me, decay_in, frequency_in, input_map_in, readout_in, paired
        )
        loads[1].wait()
        pl.semaphore_wait(barrier, tp_count - jnp.where(first_chip, 1, 0))
        gather_over_tp(
            wide, tables, rates, proj_sent, proj_got, table_sent, table_got, rate_sent, rate_got
        )

    @pl.when(jnp.logical_and(core == 0, first_chip))
    def _():
        pl.semaphore_wait(barrier, 1)
        pl.semaphore_signal(ready, inc=1, device_id=partner, device_id_type=MESH)

    loads[2].wait()

    @pl.when(jnp.logical_and(core == 1, jnp.logical_not(first_chip)))
    def _():
        pass_all()

    row = lax.broadcasted_iota(jnp.int32, (rows, LANES), 0)
    lane = lax.broadcasted_iota(jnp.int32, (rows, LANES), 1)
    step_rows = rows // LANES
    column = jnp.zeros((rows, 1), F32)
    for k in range(step_rows):
        line = step[pl.ds(me * step_rows + k, 1), :]
        column += jnp.sum(
            jnp.where(lane + k * LANES <= row, jnp.broadcast_to(line, (rows, LANES)), 0.0),
            axis=1, keepdims=True,
        )
    tau[...] = jnp.broadcast_to(column, (rows, LANES))
    loads[0].wait()
    loads[3].wait()
    strip = 16

    def norm(i, carry):
        here = pl.ds(pl.multiple_of(i * strip, strip), strip)
        value = tok[here, :].astype(F32)
        scale = lax.rsqrt(jnp.mean(value * value, axis=1, keepdims=True) + 1e-06)
        normed[here, :] = (value * scale * in_gain[...]).astype(BF16)
        return carry

    lax.fori_loop(0, rows // strip, norm, 0)
    @pl.when(core == 0)
    def _():
        pass_on(0).wait_recv()

    first_row = lax.broadcasted_iota(jnp.int32, (CHUNK, LANES), 0) == 0

    def tables_of(i, carry):
        shard, inner = i // per_shard, lax.rem(i, per_shard)
        rate = rates[shard, pl.ds(inner, 1), :]
        high, low = turns_of(rates[shard, pl.ds(per_shard + inner, 1), :])
        before_re = jnp.ones((CHUNK, LANES), F32)
        before_im = jnp.zeros((CHUNK, LANES), F32)
        for c in range(0, rows, CHUNK):
            here = pl.ds(c, CHUNK)
            times = tau[here, :]
            cosine, sine = rotation(high, low, times)
            exponent = rate * times
            shrink, grow = jnp.exp(-exponent), jnp.exp(exponent)
            e_re[i, here, :] = shrink * cosine
            e_im[i, here, :] = shrink * sine
            q_re, q_im = grow * cosine, -(grow * sine)
            turned_re, turned_im = pltpu.roll(q_re, 1, 0), pltpu.roll(q_im, 1, 0)
            g_re[i, here, :] = jnp.where(first_row, before_re, turned_re) - q_re
            g_im[i, here, :] = jnp.where(first_row, before_im, turned_im) - q_im
            before_re, before_im = turned_re, turned_im
        return carry

    lax.fori_loop(0, tiles, tables_of, 0)

    @pl.when(core == 0)
    def _():
        loads[1].wait()
        for slot in range(1, len(passed)):
            pass_on(slot).wait_recv()

    for t in range(0, shards, 2):
        both = jnp.dot(
            normed[...],
            jnp.concatenate([wide[t], wide[t + 1]], axis=1),
            preferred_element_type=F32,
        )
        drive[t] = both[:, :LANES].astype(BF16)
        drive[t + 1] = both[:, LANES:].astype(BF16)

    k_row = lax.broadcasted_iota(jnp.int32, (LANES, LANES), 0)
    k_lane = lax.broadcasted_iota(jnp.int32, (LANES, LANES), 1)
    group_rows = LANES // (2 * per_shard)

    def inject(i, half):
        shard, inner = i // per_shard, lax.rem(i, per_shard)
        mask = k_row // group_rows == 2 * inner + k_lane // CHUNK
        push = [
            jnp.where(
                mask,
                jnp.concatenate(
                    [
                        tables[
                            shard,
                            pl.ds(pl.multiple_of((2 * inner + b) * group_rows, group_rows), group_rows),
                            :,
                        ].astype(F32)
                    ]
                    * (LANES // group_rows),
                    axis=0,
                ),
                0.0,
            ).astype(BF16)
            for b in range(2)
        ]
        pushed[...] = jnp.dot(
            drive[shard], jnp.concatenate(push, axis=1), preferred_element_type=F32
        )
        sum_re = jnp.zeros((CHUNK, LANES), F32)
        sum_im = jnp.zeros((CHUNK, LANES), F32)
        for c in range(0, rows, CHUNK):
            here = pl.ds(c, CHUNK)
            u_re, u_im = pushed[here, :LANES], pushed[here, LANES:]
            a_re, a_im = g_re[i, here, :], g_im[i, here, :]
            w_re = a_re * u_re - a_im * u_im
            w_im = a_re * u_im + a_im * u_re
            sum_re += w_re
            sum_im += w_im
            inj[i, here, :LANES] = w_re.astype(BF16)
            inj[i, here, LANES:] = w_im.astype(BF16)
        t_re = jnp.sum(sum_re, axis=0, keepdims=True)
        t_im = jnp.sum(sum_im, axis=0, keepdims=True)
        d_re, d_im = e_re[i, rows - 1 : rows, :], e_im[i, rows - 1 : rows, :]
        part = i // 2
        send1[part, half : half + 1, :] = d_re * t_re - d_im * t_im
        send1[part, 2 + half : 3 + half, :] = d_re * t_im + d_im * t_re
        send1[part, 4 + half : 5 + half, :] = d_re
        send1[part, 6 + half : 7 + half, :] = d_im

    def inject_pair(part, carry):
        inject(2 * part, 0)
        inject(2 * part + 1, 1)
        return carry

    lax.fori_loop(0, tiles // 2, inject_pair, 0)

    @pl.when(jnp.logical_and(core == 1, first_chip))
    def _():
        pl.semaphore_wait(ready, 1)
        pass_all()

    @pl.when(place == hub)
    def _():
        pl.semaphore_wait(barrier, members - 1 + members * (planes - 1 - plane))
        for k in range(members):
            if k != hub:
                pl.semaphore_signal(all_in, inc=1, device_id=member(k), device_id_type=MESH)

    @pl.when(place != hub)
    def _():
        pl.semaphore_wait(all_in, 1)

    @pl.when(core == 0)
    def _():
        pass_back().start()

    def copy1(k):
        return pltpu.make_async_remote_copy(
            src_ref=send1.at[k], dst_ref=got1.at[place], send_sem=s1.at[k], recv_sem=r1.at[place],
            device_id=member(k), device_id_type=MESH,
        )

    for k in range(members):
        @pl.when(place != k)
        def _():
            copy1(k).start()

    def copy_time(z):
        return pltpu.make_async_remote_copy(
            src_ref=plane_time, dst_ref=time_got.at[plane], send_sem=st.at[z],
            recv_sem=rt.at[plane], device_id=at_plane(z), device_id_type=MESH,
        )

    @pl.when(core == 1)
    def _():
        pass_back().wait_recv()

    steps[pl.ds(core, 1)] = step[...].reshape(1, *step.shape)
    whole_plane = jnp.sum(jnp.sum(steps[0] + steps[1], axis=1, keepdims=True), axis=0, keepdims=True)
    plane_time[...] = jnp.broadcast_to(whole_plane, plane_time.shape)
    loop(plane + 1, planes, lambda z: copy_time(z).start())
    p_row = lax.broadcasted_iota(jnp.int32, (rows, rows), 0)
    p_col = lax.broadcasted_iota(jnp.int32, (rows, rows), 1)
    lower = jnp.where(p_col <= p_row, 1.0, 0.0).astype(BF16)

    def prefix(i):
        total[i] = jnp.dot(lower, inj[i], preferred_element_type=F32)

    loop(0, tiles, prefix)

    got1[pl.ds(place, 1)] = send1[pl.ds(place, 1)]
    for k in range(members):
        @pl.when(place != k)
        def _():
            pltpu.make_async_remote_copy(
                src_ref=send1.at[k], dst_ref=got1.at[k], send_sem=s1.at[k], recv_sem=r1.at[k],
                device_id=member(k), device_id_type=MESH,
            ).wait_recv()

    def advance(k, re, im):
        block = got1[k]
        d_re, d_im = block[4:6], block[6:8]
        return d_re * re - d_im * im + block[0:2], d_re * im + d_im * re + block[2:4]

    nothing = jnp.zeros((2, LANES), F32)
    re, im = nothing, nothing
    for k in range(members):
        re, im = advance(k, re, im)
    plane_end[0:2, :] = re
    plane_end[2:4, :] = im

    def copy2(z):
        return pltpu.make_async_remote_copy(
            src_ref=plane_end, dst_ref=plane_got.at[plane], send_sem=s2.at[z],
            recv_sem=r2.at[plane], device_id=at_plane(z), device_id_type=MESH,
        )

    loop(plane + 1, planes, lambda z: copy2(z).start())

    def time_wait(z):
        pltpu.make_async_remote_copy(
            src_ref=plane_time, dst_ref=time_got.at[z], send_sem=st.at[z], recv_sem=rt.at[z],
            device_id=at_plane(z), device_id_type=MESH,
        ).wait_recv()

    loop(0, plane, time_wait)

    def plane_decay(z):
        times = jnp.broadcast_to(time_got[z], (1, LANES))
        for half in range(2):
            i = 2 * place + half
            shard, inner = i // per_shard, lax.rem(i, per_shard)
            rate = rates[shard, pl.ds(inner, 1), :]
            high, low = turns_of(rates[shard, pl.ds(per_shard + inner, 1), :])
            cosine, sine = rotation(high, low, times)
            shrink = jnp.exp(-(rate * times))
            decays[z, half : half + 1, :] = shrink * cosine
            decays[z, 2 + half : 3 + half, :] = shrink * sine

    loop(0, plane, plane_decay)

    def end_wait(z):
        pltpu.make_async_remote_copy(
            src_ref=plane_end, dst_ref=plane_got.at[z], send_sem=s2.at[z], recv_sem=r2.at[z],
            device_id=at_plane(z), device_id_type=MESH,
        ).wait_recv()

    loop(0, plane, end_wait)

    def earlier(z, carry):
        re, im = carry
        d, end = decays[z], plane_got[z]
        return (
            d[0:2] * re - d[2:4] * im + end[0:2],
            d[0:2] * im + d[2:4] * re + end[2:4],
        )

    re, im = lax.fori_loop(0, plane, earlier, (nothing, nothing))
    for k in range(members):
        send3[k, 0:2, :] = re
        send3[k, 2:4, :] = im
        if k < members - 1:
            re, im = advance(k, re, im)

    def copy3(k):
        return pltpu.make_async_remote_copy(
            src_ref=send3.at[k], dst_ref=got3.at[place], send_sem=s3.at[k], recv_sem=r3.at[place],
            device_id=member(k), device_id_type=MESH,
        )

    for k in range(members):
        @pl.when(place != k)
        def _():
            copy3(k).start()
    got3[pl.ds(place, 1)] = send3[pl.ds(place, 1)]
    for k in range(members):
        @pl.when(place != k)
        def _():
            pltpu.make_async_remote_copy(
                src_ref=send3.at[k], dst_ref=got3.at[k], send_sem=s3.at[k], recv_sem=r3.at[k],
                device_id=member(k), device_id_type=MESH,
            ).wait_recv()

    answer[...] = jnp.zeros_like(answer)

    def respond(i, half):
        shard, inner = i // per_shard, lax.rem(i, per_shard)
        part = i // 2
        in_re = got3[part, half : half + 1, :]
        in_im = got3[part, 2 + half : 3 + half, :]
        for c in range(0, rows, CHUNK):
            here = pl.ds(c, CHUNK)
            a_re, a_im = total[i, here, :LANES] + in_re, total[i, here, LANES:] + in_im
            p_re, p_im = e_re[i, here, :], e_im[i, here, :]
            inj[i, here, :LANES] = (p_re * a_re - p_im * a_im).astype(BF16)
            inj[i, here, LANES:] = (p_re * a_im + p_im * a_re).astype(BF16)
        read = tables[shard, LANES:, :].astype(F32)
        lane_group = lax.broadcasted_iota(jnp.int32, (CHUNK, LANES), 1) // group_rows
        blocks = [
            jnp.where(lane_group == 2 * inner + g, read[b * CHUNK : (b + 1) * CHUNK], 0.0)
            for b in range(2)
            for g in range(2)
        ]
        answer[shard] += jnp.dot(
            inj[i], jnp.concatenate(blocks, axis=0).astype(BF16), preferred_element_type=F32
        )

    def respond_pair(part):
        respond(2 * part, 0)
        respond(2 * part + 1, 1)

    loop(0, tiles // 2, respond_pair)

    loads[4].wait()

    def finish(i):
        here = pl.ds(pl.multiple_of(i * CHUNK, CHUNK), CHUNK)
        values = []
        squares = jnp.zeros((CHUNK, LANES), F32)
        for t in range(shards):
            v = answer[t, here, :]
            v = 0.5 * v * (1.0 + jnp.tanh(0.7978845608 * (v + 0.044715 * (v * v * v))))
            v = v.astype(BF16).astype(F32)
            values.append(v)
            squares += v * v
        mean = jnp.sum(squares, axis=1, keepdims=True) * np.float32(1.0 / (shards * LANES))
        scale = lax.rsqrt(mean + 1e-06)
        for t in range(shards):
            line = pl.ds(t * LANES, LANES)
            shaped[here, line] = (values[t] * scale * out_gain[:, line]).astype(BF16)

    loop(0, rows // CHUNK, finish)

    for k in range(members):
        @pl.when(place != k)
        def _():
            copy1(k).wait_send()
            copy3(k).wait_send()
    loop(plane + 1, planes, lambda z: copy_time(z).wait_send())
    loop(plane + 1, planes, lambda z: copy2(z).wait_send())

    @pl.when(core == 1)
    def _():
        for slot in range(len(passed)):
            pass_on(slot).wait_send()

    @pl.when(core == 0)
    def _():
        pass_back().wait_send()


def mix(tokens, proj, decay, frequency, input_map, readout, step, in_gain, out_gain):
    rows, width = tokens.shape
    shards = lax.axis_size("tp")
    planes = lax.axis_size("sp") // 2
    members = 2 * shards
    pairs = decay.size // LANES
    tiles = shards * pairs
    vmem = pl.BlockSpec(memory_space=pltpu.VMEM)
    far = pl.BlockSpec(memory_space=pltpu.HBM)
    table = pltpu.VMEM((tiles, rows, LANES), F32)
    dma = pltpu.SemaphoreType.DMA
    passed = shards + 3
    return pl.pallas_call(
        mixer_kernel,
        out_shape=jax.ShapeDtypeStruct((rows, shards * LANES), BF16),
        in_specs=[far] * 9,
        out_specs=vmem,
        scratch_shapes=[
            pltpu.VMEM(tokens.shape, BF16),
            pltpu.VMEM((shards, *proj.shape), BF16),
            pltpu.VMEM((shards, 2 * LANES, LANES), BF16),
            pltpu.VMEM((shards, 2 * pairs, LANES), F32),
            pltpu.VMEM((2, *step.shape), F32),
            *(pltpu.VMEM(a.shape, F32) for a in (step, in_gain, out_gain)),
            *(pltpu.VMEM(a.shape, F32) for a in (decay, frequency, input_map, readout)),
            pltpu.VMEM((2, pairs, input_map.shape[2], LANES), F32),
            pltpu.VMEM(tokens.shape, BF16),
            pltpu.VMEM((shards, rows, LANES), BF16),
            table, table, table, table,
            pltpu.VMEM((tiles, rows, 2 * LANES), BF16),
            pltpu.VMEM((rows, 2 * LANES), F32),
            pltpu.VMEM((tiles, rows, 2 * LANES), F32),
            pltpu.VMEM((shards, rows, LANES), F32),
            pltpu.VMEM((rows, LANES), F32),
            pltpu.VMEM((members, 8, LANES), F32),
            pltpu.VMEM((members, 8, LANES), F32),
            pltpu.VMEM((planes, 4, LANES), F32),
            pltpu.VMEM((4, LANES), F32),
            pltpu.VMEM((planes, 4, LANES), F32),
            pltpu.VMEM((1, LANES), F32),
            pltpu.VMEM((planes, 1, LANES), F32),
            pltpu.VMEM((members, 4, LANES), F32),
            pltpu.VMEM((members, 4, LANES), F32),
            dma((9,)),
            dma((members,)), dma((members,)),
            dma((planes,)), dma((planes,)),
            dma((planes,)), dma((planes,)),
            dma((members,)), dma((members,)),
            dma((6,)), dma((6,)), dma((6,)), dma((6,)), dma((3,)), dma((3,)),
            dma((passed,)), dma((passed,)),
            pltpu.SemaphoreType.REGULAR,
            pltpu.SemaphoreType.REGULAR,
        ],
        compiler_params=pltpu.CompilerParams(
            collective_id=0, has_side_effects=True, vmem_limit_bytes=48 << 20
        ),
        name="mixer",
    )(
        *(
            pltpu.with_memory_space_constraint(a, pltpu.HBM)
            for a in (tokens, proj, decay, frequency, input_map, readout, step, in_gain, out_gain)
        )
    )


def on_device(
    tokens, step, in_gain, in_proj, decay_rate, frequency, input_map, readout, out_gain, out_proj
):
    shaped = mix(
        tokens, in_proj, decay_rate, frequency, jnp.swapaxes(input_map, 2, 3), readout,
        step.reshape(-1, LANES), in_gain.reshape(1, -1), out_gain.reshape(1, -1),
    )
    return jnp.dot(shaped, out_proj, preferred_element_type=F32).astype(BF16)


def solution(mesh):
    placed = (
        P(("grp", "sp", "tp"), None),
        P(("grp", "sp")),
        P(),
        P(None, "tp"),
        P("tp", None),
        P("tp", None),
        P(None, "tp", None, None),
        P(None, "tp", None, None),
        P(),
        P(),
    )
    return jax.shard_map(
        on_device,
        mesh=mesh,
        in_specs=placed,
        out_specs=P(("grp", "sp", "tp"), None),
        check_vma=False,
    )
```

```python
import functools

import jax
import jax.numpy as jnp
import numpy as np
from jax import lax
from jax.experimental import pallas as pl
from jax.experimental.pallas import tpu as pltpu
from jax.sharding import PartitionSpec as P

F32, BF16 = jnp.float32, jnp.bfloat16
MESH = pl.DeviceIdType.MESH
LANES = 128
CHUNK = 64
BLOCK = 8
SIN = (6.283182782944718, -41.34141729070845, 81.59606953187966, -76.57887013158442, 41.19977042473147, -12.262090350994187)
COS = (0.9999992033069715, -19.738978121285577, 64.92856232184074, -85.27029302060335, 58.78321908130333, -21.057556163478825)
TURN = np.float32(1.0 / (2.0 * np.pi))
TURN_LOW = np.float32(1.0 / (2.0 * np.pi) - float(TURN))


def halves(value):
    wide = value * np.float32(4097.0)
    high = wide - (wide - value)
    return high, value - high


def turns_of(freqs):
    high = freqs * TURN
    f_high, f_low = halves(freqs)
    c_high, c_low = (np.float32(v) for v in halves(TURN))
    error = ((f_high * c_high - high) + f_high * c_low + f_low * c_high) + f_low * c_low
    return high, error + freqs * TURN_LOW


def polynomial(x, terms):
    total = jnp.full_like(x, np.float32(terms[-1]))
    for term in terms[-2::-1]:
        total = total * x + np.float32(term)
    return total


def rotation(high, low, times):
    whole = high * times
    part = (whole - jnp.round(whole)) + low * times
    square = part * part
    return polynomial(square, COS), polynomial(square, [-c for c in SIN]) * part


def gather_over_tp(wide, tables, rates, proj_sent, proj_got, table_sent, table_got, rate_sent, rate_got):
    count, me = lax.axis_size("tp"), lax.axis_index("tp")
    right, left, across = (lax.rem(me + k, count) for k in (1, count - 1, 2))

    def piece(k, shard, half, slot, target):
        ref, sent, got = ((wide, proj_sent, proj_got), (tables, table_sent, table_got))[k]
        size = ref.shape[1] // 2
        where = ref.at[shard, pl.ds(half * size, size)]
        return pltpu.make_async_remote_copy(
            src_ref=where, dst_ref=where, send_sem=sent.at[slot], recv_sem=got.at[slot],
            device_id={"tp": target}, device_id_type=MESH,
        )

    started = []

    def go(copy):
        copy.start()
        started.append(copy)

    small = [
        pltpu.make_async_remote_copy(
            src_ref=rates.at[me], dst_ref=rates.at[me], send_sem=rate_sent.at[slot],
            recv_sem=rate_got.at[slot], device_id={"tp": target}, device_id_type=MESH,
        )
        for slot, target in enumerate((right, left, across))
    ]
    for copy in small:
        go(copy)
    for order in range(2):
        for k in (1, 0):
            go(piece(k, me, order, order, right))
            go(piece(k, me, 1 - order, 2 + order, left))
    for shard, half, slot, onward, onward_slot in (
        (left, 0, 0, right, 4),
        (right, 1, 2, left, 5),
        (left, 1, 1, None, None),
        (right, 0, 3, None, None),
        (across, 0, 4, None, None),
        (across, 1, 5, None, None),
    ):
        for k in (1, 0):
            piece(k, shard, half, slot, left).wait_recv()
            if onward is not None:
                go(piece(k, shard, half, onward_slot, onward))
    for copy in small:
        copy.wait_recv()
    for copy in started:
        copy.wait_send()


def own_tables(tables, rates, me, decay, frequency, input_map, readout, paired):
    groups, states = decay.shape
    channels = input_map.shape[-2]
    pairs = groups // 2
    for g in range(groups):
        lanes = slice((g % 2) * states, (g % 2 + 1) * states)
        rates[me, g // 2 : g // 2 + 1, lanes] = decay[g : g + 1, :]
        rates[me, pairs + g // 2 : pairs + g // 2 + 1, lanes] = frequency[g : g + 1, :]
        for c in range(2):
            paired[c, g // 2, :, lanes] = input_map[c, g]
            paired[2 + c, g // 2, :, lanes] = readout[c, g]
    for k in range(pairs):
        lam_re = -rates[me, k : k + 1, :]
        lam_im = rates[me, pairs + k : pairs + k + 1, :]
        size = lam_re * lam_re + lam_im * lam_im
        m_re, m_im = paired[0, k], paired[1, k]
        for b, value in enumerate(
            (
                (m_re * lam_re + m_im * lam_im) / size,
                (m_im * lam_re - m_re * lam_im) / size,
                paired[2, k],
                -paired[3, k],
            )
        ):
            at = (b // 2) * LANES + (2 * k + b % 2) * channels
            tables[me, at : at + channels, :] = value.astype(BF16)


def mixer_kernel(
    tokens, proj, decay, frequency, input_map, readout, step_hbm, in_gain_hbm, out_gain_hbm, shaped,
    tok, wide, tables, rates, steps, step, in_gain, out_gain,
    decay_in, frequency_in, input_map_in, readout_in, paired,
    normed, drive, q_re, q_im, g_re, g_im, inj, back, pushed, answer, tau,
    send1, got1, decays, plane_end, plane_got, plane_time, time_got, send3, got3,
    block_end, block_got, block_in,
    load, s1, r1, s2, r2, st, rt, s3, r3,
    proj_sent, proj_got, table_sent, table_got, rate_sent, rate_got, pass_sent, pass_got,
    sb, rb, ready, all_in,
):
    rows = tok.shape[0]
    tp_count, sp_count = lax.axis_size("tp"), lax.axis_size("sp")
    planes = sp_count // 2
    members = 2 * tp_count
    me, sp = lax.axis_index("tp"), lax.axis_index("sp")
    core, plane = lax.rem(sp, 2), sp // 2
    first = plane - lax.rem(plane, BLOCK)
    stop = jnp.minimum(first + BLOCK, planes)
    reach = jnp.where(plane == stop - 1, jnp.minimum(stop + BLOCK, planes), stop)
    place = core * tp_count + me
    tiles = q_re.shape[0]
    per_shard = tiles // tp_count
    shards = tp_count

    def member(k):
        return {"sp": plane * 2 + k // tp_count, "tp": k % tp_count}

    def at_plane(z):
        return {"sp": z * 2 + core}

    partner = {"sp": sp + 1 - 2 * core}

    def loop(lower, upper, body):
        def step(z, carry):
            body(z)
            return carry

        lax.fori_loop(lower, upper, step, 0)

    hub, gate = 1, 2
    first_chip = me == 0
    barrier = pltpu.get_barrier_semaphore()

    def greet(target):
        pl.semaphore_signal(barrier, inc=1, device_id=target, device_id_type=MESH)

    loads = [
        pltpu.make_async_copy(src, dst, load.at[k])
        for k, (src, dst) in enumerate(
            (
                (tokens, tok),
                (proj, wide.at[me]),
                (step_hbm, step),
                (in_gain_hbm, in_gain),
                (out_gain_hbm, out_gain),
            )
        )
    ]

    @pl.when(core == 1)
    def _():
        for k in range(1, tp_count):
            greet({"tp": lax.rem(me + k, tp_count)})

    @pl.when((core == 0) != first_chip)
    def _():
        greet(partner)

    @pl.when(place != hub)
    def _():
        greet(member(hub))

    for k in (2, 0, 1, 3, 4):
        loads[k].start()

    def plane_in():
        pl.semaphore_wait(barrier, members - 1)
        greet(member(gate))
        loop(jnp.maximum(first - 1, 0), plane, lambda z: greet({"sp": 2 * z, "tp": gate}))

    @pl.when(jnp.logical_and(place == hub, plane > 0))
    def _():
        plane_in()

    passed = [
        (rates, rates),
        (tables, tables),
        *((wide.at[lax.rem(me + k, tp_count)],) * 2 for k in range(1, tp_count)),
        (step, steps.at[1]),
    ]

    def pass_on(slot):
        src, dst = passed[slot]
        return pltpu.make_async_remote_copy(
            src_ref=src, dst_ref=dst, send_sem=pass_sent.at[slot], recv_sem=pass_got.at[slot],
            device_id=partner, device_id_type=MESH,
        )

    def pass_back():
        slot = len(passed)
        return pltpu.make_async_remote_copy(
            src_ref=step, dst_ref=steps.at[0], send_sem=pass_sent.at[slot],
            recv_sem=pass_got.at[slot], device_id=partner, device_id_type=MESH,
        )

    def pass_all():
        for slot in (0, *range(2, len(passed)), 1):
            pass_on(slot).start()

    @pl.when(core == 1)
    def _():
        inward = [
            pltpu.make_async_copy(src, dst, load.at[len(loads) + k])
            for k, (src, dst) in enumerate(
                (
                    (decay, decay_in),
                    (frequency, frequency_in),
                    (input_map, input_map_in),
                    (readout, readout_in),
                )
            )
        ]
        for copy in inward:
            copy.start()
        for copy in inward:
            copy.wait()
        own_tables(
            tables, rates, me, decay_in, frequency_in, input_map_in, readout_in, paired
        )
        loads[1].wait()
        pl.semaphore_wait(barrier, tp_count - jnp.where(first_chip, 1, 0))
        gather_over_tp(
            wide, tables, rates, proj_sent, proj_got, table_sent, table_got, rate_sent, rate_got
        )

    @pl.when(jnp.logical_and(core == 0, first_chip))
    def _():
        pl.semaphore_wait(barrier, 1)
        pl.semaphore_signal(ready, inc=1, device_id=partner, device_id_type=MESH)

    loads[2].wait()

    @pl.when(jnp.logical_and(core == 1, jnp.logical_not(first_chip)))
    def _():
        pass_all()

    row = lax.broadcasted_iota(jnp.int32, (rows, LANES), 0)
    lane = lax.broadcasted_iota(jnp.int32, (rows, LANES), 1)
    step_rows = rows // LANES
    column = jnp.zeros((rows, 1), F32)
    for k in range(step_rows):
        line = step[pl.ds(me * step_rows + k, 1), :]
        column += jnp.sum(
            jnp.where(lane + k * LANES <= row, jnp.broadcast_to(line, (rows, LANES)), 0.0),
            axis=1, keepdims=True,
        )
    tau[...] = jnp.broadcast_to(column, (rows, LANES))
    loads[0].wait()
    loads[3].wait()
    strip = 16

    def norm(i, carry):
        here = pl.ds(pl.multiple_of(i * strip, strip), strip)
        value = tok[here, :].astype(F32)
        scale = lax.rsqrt(jnp.mean(value * value, axis=1, keepdims=True) + 1e-06)
        normed[here, :] = (value * scale * in_gain[...]).astype(BF16)
        return carry

    lax.fori_loop(0, rows // strip, norm, 0)
    @pl.when(core == 0)
    def _():
        pass_on(0).wait_recv()

    first_row = lax.broadcasted_iota(jnp.int32, (8, LANES), 0) == 0

    def rate_row(i):
        return rates[i // per_shard, pl.ds(lax.rem(i, per_shard), 1), :]

    def turn_rows(i):
        return turns_of(rates[i // per_shard, pl.ds(per_shard + lax.rem(i, per_shard), 1), :])

    def tables_of(i, carry):
        rate, (high, low) = rate_row(i), turn_rows(i)
        before = [jnp.ones((8, LANES), F32), jnp.zeros((8, LANES), F32)]
        for c in range(0, rows, CHUNK):
            here = pl.ds(c, CHUNK)
            times = tau[here, :]
            grow = jnp.exp(rate * times)
            for b, (part, q_ref, g_ref) in enumerate(
                zip(rotation(high, low, times), (q_re, q_im), (g_re, g_im))
            ):
                value = grow * part
                q_ref[i, here, :] = value
                turned = pltpu.roll(value, 1, 0)
                head = jnp.where(first_row, before[b], turned[:8])
                before[b] = turned[:8]
                g_ref[i, here, :] = jnp.concatenate([head, turned[8:]], axis=0) - value
        return carry

    lax.fori_loop(0, tiles, tables_of, 0)

    @pl.when(core == 0)
    def _():
        loads[1].wait()
        for slot in range(1, len(passed)):
            pass_on(slot).wait_recv()

    for t in range(0, shards, 2):
        both = jnp.dot(
            normed[...],
            jnp.concatenate([wide[t], wide[t + 1]], axis=1),
            preferred_element_type=F32,
        )
        drive[t] = both[:, :LANES].astype(BF16)
        drive[t + 1] = both[:, LANES:].astype(BF16)

    k_row = lax.broadcasted_iota(jnp.int32, (LANES, LANES), 0)
    k_lane = lax.broadcasted_iota(jnp.int32, (LANES, LANES), 1)
    group_rows = LANES // (2 * per_shard)

    def own_groups(inner):
        return k_row // group_rows == 2 * inner + k_lane // (LANES // 2)

    def compact(shard, block):
        at = pl.multiple_of(block * group_rows, group_rows)
        return tables[shard, pl.ds(at, group_rows), :].astype(F32)

    def widened(value, mask):
        return jnp.where(mask, jnp.concatenate([value] * (LANES // group_rows), axis=0), 0.0).astype(
            BF16
        )

    def spread(shard, block, mask):
        return widened(compact(shard, block), mask)

    def inject(i, half):
        shard, inner = i // per_shard, lax.rem(i, per_shard)
        mask = own_groups(inner)
        push = [spread(shard, 2 * inner + b, mask) for b in range(2)]
        pushed[...] = jnp.dot(
            drive[shard], jnp.concatenate(push, axis=1), preferred_element_type=F32
        )
        sum_re = jnp.zeros((CHUNK, LANES), F32)
        sum_im = jnp.zeros((CHUNK, LANES), F32)
        for c in range(0, rows, CHUNK):
            here = pl.ds(c, CHUNK)
            u_re, u_im = pushed[here, :LANES], pushed[here, LANES:]
            a_re, a_im = g_re[i, here, :], g_im[i, here, :]
            w_re = a_re * u_re - a_im * u_im
            w_im = a_re * u_im + a_im * u_re
            sum_re += w_re
            sum_im += w_im
            inj[i, here, :LANES] = w_re.astype(BF16)
            inj[i, here, LANES:] = w_im.astype(BF16)
        t_re = jnp.sum(sum_re, axis=0, keepdims=True)
        t_im = jnp.sum(sum_im, axis=0, keepdims=True)
        fade = jnp.exp(-2.0 * (rate_row(i) * tau[rows - 1 : rows, :]))
        d_re, d_im = q_re[i, rows - 1 : rows, :] * fade, -(q_im[i, rows - 1 : rows, :] * fade)
        part = i // 2
        send1[part, half : half + 1, :] = d_re * t_re - d_im * t_im
        send1[part, 2 + half : 3 + half, :] = d_re * t_im + d_im * t_re
        send1[part, 4 + half : 5 + half, :] = d_re
        send1[part, 6 + half : 7 + half, :] = d_im

    def inject_pair(part, carry):
        inject(2 * part, 0)
        inject(2 * part + 1, 1)
        return carry

    lax.fori_loop(0, tiles // 2, inject_pair, 0)

    @pl.when(jnp.logical_and(core == 1, first_chip))
    def _():
        pl.semaphore_wait(ready, 1)
        pass_all()

    @pl.when(jnp.logical_and(place == hub, plane == 0))
    def _():
        plane_in()

    @pl.when(place == gate)
    def _():
        pl.semaphore_wait(barrier, reach - plane)
        for k in range(members):
            if k != gate:
                pl.semaphore_signal(all_in, inc=1, device_id=member(k), device_id_type=MESH)

    @pl.when(place != gate)
    def _():
        pl.semaphore_wait(all_in, 1)

    @pl.when(core == 0)
    def _():
        pass_back().start()

    def copy1(k):
        return pltpu.make_async_remote_copy(
            src_ref=send1.at[k], dst_ref=got1.at[place], send_sem=s1.at[k], recv_sem=r1.at[place],
            device_id=member(k), device_id_type=MESH,
        )

    for k in range(members):
        @pl.when(place != k)
        def _():
            copy1(k).start()

    def copy_time(z):
        return pltpu.make_async_remote_copy(
            src_ref=plane_time, dst_ref=time_got.at[plane], send_sem=st.at[z],
            recv_sem=rt.at[plane], device_id=at_plane(z), device_id_type=MESH,
        )

    @pl.when(core == 1)
    def _():
        pass_back().wait_recv()

    steps[pl.ds(core, 1)] = step[...].reshape(1, *step.shape)
    whole_plane = jnp.sum(jnp.sum(steps[0] + steps[1], axis=1, keepdims=True), axis=0, keepdims=True)
    plane_time[...] = jnp.broadcast_to(whole_plane, plane_time.shape)
    loop(plane + 1, stop, lambda z: copy_time(z).start())
    p_row = lax.broadcasted_iota(jnp.int32, (rows, rows), 0)
    p_col = lax.broadcasted_iota(jnp.int32, (rows, rows), 1)
    lower = jnp.where(p_col <= p_row, 1.0, 0.0).astype(BF16)

    blocks = LANES // group_rows

    def across(left, right):
        return lax.dot_general(
            left, right, (((1,), (1,)), ((), ())), preferred_element_type=F32
        )

    def prefix(i, first):
        shard, inner = i // per_shard, lax.rem(i, per_shard)
        pushed[...] = jnp.dot(lower, inj[i], preferred_element_type=F32)
        rate = rate_row(i)
        for c in range(0, rows, CHUNK):
            here = pl.ds(c, CHUNK)
            fade = jnp.exp(-2.0 * (rate * tau[here, :]))
            e_re, e_im = q_re[i, here, :] * fade, -(q_im[i, here, :] * fade)
            a_re, a_im = pushed[here, :LANES], pushed[here, LANES:]
            back[i, here, :LANES] = e_re.astype(BF16)
            back[i, here, LANES:] = e_im.astype(BF16)
            inj[i, here, :LANES] = (e_re * a_re - e_im * a_im).astype(BF16)
            inj[i, here, LANES:] = (e_re * a_im + e_im * a_re).astype(BF16)
        mask = own_groups(inner)
        read = [spread(shard, blocks + 2 * inner + b, mask) for b in range(2)]
        value = across(inj[i], jnp.concatenate(read, axis=1))
        if first:
            answer[shard] = value
        else:
            answer[shard] += value

    def prefixes(shard):
        for inner in range(per_shard):
            prefix(shard * per_shard + inner, inner == 0)

    loop(0, shards, prefixes)

    got1[pl.ds(place, 1)] = send1[pl.ds(place, 1)]
    for k in range(members):
        @pl.when(place != k)
        def _():
            pltpu.make_async_remote_copy(
                src_ref=send1.at[k], dst_ref=got1.at[k], send_sem=s1.at[k], recv_sem=r1.at[k],
                device_id=member(k), device_id_type=MESH,
            ).wait_recv()

    def advance(k, re, im):
        block = got1[k]
        d_re, d_im = block[4:6], block[6:8]
        return d_re * re - d_im * im + block[0:2], d_re * im + d_im * re + block[2:4]

    nothing = jnp.zeros((2, LANES), F32)
    re, im = nothing, nothing
    for k in range(members):
        re, im = advance(k, re, im)
    plane_end[0:2, :] = re
    plane_end[2:4, :] = im

    def copy2(z):
        return pltpu.make_async_remote_copy(
            src_ref=plane_end, dst_ref=plane_got.at[plane], send_sem=s2.at[z],
            recv_sem=r2.at[plane], device_id=at_plane(z), device_id_type=MESH,
        )

    loop(plane + 1, stop, lambda z: copy2(z).start())

    def time_wait(z):
        pltpu.make_async_remote_copy(
            src_ref=plane_time, dst_ref=time_got.at[z], send_sem=st.at[z], recv_sem=rt.at[z],
            device_id=at_plane(z), device_id_type=MESH,
        ).wait_recv()

    loop(first, plane, time_wait)

    def plane_decay(z):
        times = jnp.broadcast_to(time_got[z], (1, LANES))
        for half in range(2):
            i = 2 * place + half
            rate, (high, low) = rate_row(i), turn_rows(i)
            cosine, sine = rotation(high, low, times)
            shrink = jnp.exp(-(rate * times))
            decays[z, half : half + 1, :] = shrink * cosine
            decays[z, 2 + half : 3 + half, :] = -(shrink * sine)

    loop(first, plane, plane_decay)

    def end_wait(z):
        pltpu.make_async_remote_copy(
            src_ref=plane_end, dst_ref=plane_got.at[z], send_sem=s2.at[z], recv_sem=r2.at[z],
            device_id=at_plane(z), device_id_type=MESH,
        ).wait_recv()

    loop(first, plane, end_wait)

    def earlier(z, carry):
        re, im = carry
        d, end = decays[z], plane_got[z]
        return (
            d[0:2] * re - d[2:4] * im + end[0:2],
            d[0:2] * im + d[2:4] * re + end[2:4],
        )

    def copy_block(z):
        return pltpu.make_async_remote_copy(
            src_ref=block_end, dst_ref=block_got, send_sem=sb.at[z], recv_sem=rb,
            device_id=at_plane(z), device_id_type=MESH,
        )

    @pl.when(first == 0)
    def _():
        block_in[...] = jnp.zeros_like(block_in)

    @pl.when(first > 0)
    def _():
        copy_block(plane).wait_recv()
        block_in[...] = block_got[...]

    re, im = lax.fori_loop(first, plane, earlier, (block_in[0:2, :], block_in[2:4, :]))

    @pl.when(reach > stop)
    def _():
        after_re, after_im = re, im
        for k in range(members):
            after_re, after_im = advance(k, after_re, after_im)
        block_end[0:2, :] = after_re
        block_end[2:4, :] = after_im

    loop(stop, reach, lambda z: copy_block(z).start())
    for k in range(members):
        send3[k, 0:2, :] = re
        send3[k, 2:4, :] = im
        if k < members - 1:
            re, im = advance(k, re, im)

    def copy3(k):
        return pltpu.make_async_remote_copy(
            src_ref=send3.at[k], dst_ref=got3.at[place], send_sem=s3.at[k], recv_sem=r3.at[place],
            device_id=member(k), device_id_type=MESH,
        )

    for k in range(members):
        @pl.when(place != k)
        def _():
            copy3(k).start()
    got3[pl.ds(place, 1)] = send3[pl.ds(place, 1)]
    for k in range(members):
        @pl.when(place != k)
        def _():
            pltpu.make_async_remote_copy(
                src_ref=send3.at[k], dst_ref=got3.at[k], send_sem=s3.at[k], recv_sem=r3.at[k],
                device_id=member(k), device_id_type=MESH,
            ).wait_recv()

    def respond(shard):
        value = answer[shard]
        for inner in range(per_shard):
            i = shard * per_shard + inner
            part, half = i // 2, inner % 2
            in_re = got3[part, half : half + 1, :]
            in_im = got3[part, 2 + half : 3 + half, :]
            c_re, c_im = (compact(shard, blocks + 2 * inner + b) for b in range(2))
            mask = own_groups(inner)
            read = [
                widened(c_re * in_re + c_im * in_im, mask),
                widened(c_im * in_re - c_re * in_im, mask),
            ]
            value += across(back[i], jnp.concatenate(read, axis=1))
        answer[shard] = value

    loop(0, shards, respond)

    loads[4].wait()

    def finish(i):
        here = pl.ds(pl.multiple_of(i * CHUNK, CHUNK), CHUNK)
        values = []
        squares = jnp.zeros((CHUNK, LANES), F32)
        for t in range(shards):
            v = answer[t, here, :]
            v = 0.5 * v * (1.0 + jnp.tanh(0.7978845608 * (v + 0.044715 * (v * v * v))))
            v = v.astype(BF16).astype(F32)
            values.append(v)
            squares += v * v
        mean = jnp.sum(squares, axis=1, keepdims=True) * np.float32(1.0 / (shards * LANES))
        scale = lax.rsqrt(mean + 1e-06)
        for t in range(shards):
            line = pl.ds(t * LANES, LANES)
            shaped[here, line] = (values[t] * scale * out_gain[:, line]).astype(BF16)

    loop(0, rows // CHUNK, finish)

    for k in range(members):
        @pl.when(place != k)
        def _():
            copy1(k).wait_send()
            copy3(k).wait_send()
    loop(plane + 1, stop, lambda z: copy_time(z).wait_send())
    loop(plane + 1, stop, lambda z: copy2(z).wait_send())
    loop(stop, reach, lambda z: copy_block(z).wait_send())

    @pl.when(core == 1)
    def _():
        for slot in range(len(passed)):
            pass_on(slot).wait_send()

    @pl.when(core == 0)
    def _():
        pass_back().wait_send()


def mix(tokens, proj, decay, frequency, input_map, readout, step, in_gain, out_gain):
    rows, width = tokens.shape
    shards = lax.axis_size("tp")
    planes = lax.axis_size("sp") // 2
    members = 2 * shards
    pairs = decay.size // LANES
    tiles = shards * pairs
    vmem = pl.BlockSpec(memory_space=pltpu.VMEM)
    far = pl.BlockSpec(memory_space=pltpu.HBM)
    table = pltpu.VMEM((tiles, rows, LANES), F32)
    dma = pltpu.SemaphoreType.DMA
    passed = shards + 3
    return pl.pallas_call(
        mixer_kernel,
        out_shape=jax.ShapeDtypeStruct((rows, shards * LANES), BF16),
        in_specs=[far] * 9,
        out_specs=vmem,
        scratch_shapes=[
            pltpu.VMEM(tokens.shape, BF16),
            pltpu.VMEM((shards, *proj.shape), BF16),
            pltpu.VMEM((shards, 2 * LANES, LANES), BF16),
            pltpu.VMEM((shards, 2 * pairs, LANES), F32),
            pltpu.VMEM((2, *step.shape), F32),
            *(pltpu.VMEM(a.shape, F32) for a in (step, in_gain, out_gain)),
            *(pltpu.VMEM(a.shape, F32) for a in (decay, frequency, input_map, readout)),
            pltpu.VMEM((4, pairs, input_map.shape[2], LANES), F32),
            pltpu.VMEM(tokens.shape, BF16),
            pltpu.VMEM((shards, rows, LANES), BF16),
            table, table, table, table,
            pltpu.VMEM((tiles, rows, 2 * LANES), BF16),
            pltpu.VMEM((tiles, rows, 2 * LANES), BF16),
            pltpu.VMEM((rows, 2 * LANES), F32),
            pltpu.VMEM((shards, rows, LANES), F32),
            pltpu.VMEM((rows, LANES), F32),
            pltpu.VMEM((members, 8, LANES), F32),
            pltpu.VMEM((members, 8, LANES), F32),
            pltpu.VMEM((planes, 4, LANES), F32),
            pltpu.VMEM((4, LANES), F32),
            pltpu.VMEM((planes, 4, LANES), F32),
            pltpu.VMEM((1, LANES), F32),
            pltpu.VMEM((planes, 1, LANES), F32),
            pltpu.VMEM((members, 4, LANES), F32),
            pltpu.VMEM((members, 4, LANES), F32),
            pltpu.VMEM((4, LANES), F32),
            pltpu.VMEM((4, LANES), F32),
            pltpu.VMEM((4, LANES), F32),
            dma((9,)),
            dma((members,)), dma((members,)),
            dma((planes,)), dma((planes,)),
            dma((planes,)), dma((planes,)),
            dma((members,)), dma((members,)),
            dma((6,)), dma((6,)), dma((6,)), dma((6,)), dma((3,)), dma((3,)),
            dma((passed,)), dma((passed,)),
            dma((planes,)), dma,
            pltpu.SemaphoreType.REGULAR,
            pltpu.SemaphoreType.REGULAR,
        ],
        compiler_params=pltpu.CompilerParams(
            collective_id=0, has_side_effects=True, vmem_limit_bytes=48 << 20
        ),
        name="mixer",
    )(
        *(
            pltpu.with_memory_space_constraint(a, pltpu.HBM)
            for a in (tokens, proj, decay, frequency, input_map, readout, step, in_gain, out_gain)
        )
    )


def on_device(
    tokens, step, in_gain, in_proj, decay_rate, frequency, input_map, readout, out_gain, out_proj
):
    shaped = mix(
        tokens, in_proj, decay_rate, frequency, jnp.swapaxes(input_map, 2, 3), readout,
        step.reshape(-1, LANES), in_gain.reshape(1, -1), out_gain.reshape(1, -1),
    )
    return jnp.dot(shaped, out_proj, preferred_element_type=F32).astype(BF16)


def solution(mesh):
    placed = (
        P(("grp", "sp", "tp"), None),
        P(("grp", "sp")),
        P(),
        P(None, "tp"),
        P("tp", None),
        P("tp", None),
        P(None, "tp", None, None),
        P(None, "tp", None, None),
        P(),
        P(),
    )
    return jax.shard_map(
        on_device,
        mesh=mesh,
        in_specs=placed,
        out_specs=P(("grp", "sp", "tp"), None),
        check_vma=False,
    )
```

```python
import functools

import jax
import jax.numpy as jnp
import numpy as np
from jax import lax
from jax.experimental import pallas as pl
from jax.experimental.pallas import tpu as pltpu
from jax.sharding import PartitionSpec as P

F32, BF16 = jnp.float32, jnp.bfloat16
MESH = pl.DeviceIdType.MESH
LANES = 128
CHUNK = 64
BLOCK = 4
SIN = (6.283182782944718, -41.34141729070845, 81.59606953187966, -76.57887013158442, 41.19977042473147, -12.262090350994187)
COS = (0.9999992033069715, -19.738978121285577, 64.92856232184074, -85.27029302060335, 58.78321908130333, -21.057556163478825)
TURN = np.float32(1.0 / (2.0 * np.pi))
TURN_LOW = np.float32(1.0 / (2.0 * np.pi) - float(TURN))


def halves(value):
    wide = value * np.float32(4097.0)
    high = wide - (wide - value)
    return high, value - high


def turns_of(freqs):
    high = freqs * TURN
    f_high, f_low = halves(freqs)
    c_high, c_low = (np.float32(v) for v in halves(TURN))
    error = ((f_high * c_high - high) + f_high * c_low + f_low * c_high) + f_low * c_low
    return high, error + freqs * TURN_LOW


def polynomial(x, terms):
    total = jnp.full_like(x, np.float32(terms[-1]))
    for term in terms[-2::-1]:
        total = total * x + np.float32(term)
    return total


def rotation(high, low, times):
    whole = high * times
    part = (whole - jnp.round(whole)) + low * times
    square = part * part
    return polynomial(square, COS), polynomial(square, [-c for c in SIN]) * part


def gather_over_tp(wide, tables, rates, proj_sent, proj_got, table_sent, table_got, rate_sent, rate_got):
    count, me = lax.axis_size("tp"), lax.axis_index("tp")
    right, left, across = (lax.rem(me + k, count) for k in (1, count - 1, 2))

    def piece(k, shard, half, slot, target):
        ref, sent, got = ((wide, proj_sent, proj_got), (tables, table_sent, table_got))[k]
        size = ref.shape[1] // 2
        where = ref.at[shard, pl.ds(half * size, size)]
        return pltpu.make_async_remote_copy(
            src_ref=where, dst_ref=where, send_sem=sent.at[slot], recv_sem=got.at[slot],
            device_id={"tp": target}, device_id_type=MESH,
        )

    started = []

    def go(copy):
        copy.start()
        started.append(copy)

    small = [
        pltpu.make_async_remote_copy(
            src_ref=rates.at[me], dst_ref=rates.at[me], send_sem=rate_sent.at[slot],
            recv_sem=rate_got.at[slot], device_id={"tp": target}, device_id_type=MESH,
        )
        for slot, target in enumerate((right, left, across))
    ]
    for copy in small:
        go(copy)
    for order in range(2):
        for k in (1, 0):
            go(piece(k, me, order, order, right))
            go(piece(k, me, 1 - order, 2 + order, left))
    for shard, half, slot, onward, onward_slot in (
        (left, 0, 0, right, 4),
        (right, 1, 2, left, 5),
        (left, 1, 1, None, None),
        (right, 0, 3, None, None),
        (across, 0, 4, None, None),
        (across, 1, 5, None, None),
    ):
        for k in (1, 0):
            piece(k, shard, half, slot, left).wait_recv()
            if onward is not None:
                go(piece(k, shard, half, onward_slot, onward))
    for copy in small:
        copy.wait_recv()
    for copy in started:
        copy.wait_send()


def own_tables(tables, rates, me, decay, frequency, input_map, readout, paired):
    groups, states = decay.shape
    channels = input_map.shape[-2]
    pairs = groups // 2
    for g in range(groups):
        lanes = slice((g % 2) * states, (g % 2 + 1) * states)
        rates[me, g // 2 : g // 2 + 1, lanes] = decay[g : g + 1, :]
        rates[me, pairs + g // 2 : pairs + g // 2 + 1, lanes] = frequency[g : g + 1, :]
        for c in range(2):
            paired[c, g // 2, :, lanes] = input_map[c, g]
            paired[2 + c, g // 2, :, lanes] = readout[c, g]
    for k in range(pairs):
        lam_re = -rates[me, k : k + 1, :]
        lam_im = rates[me, pairs + k : pairs + k + 1, :]
        size = lam_re * lam_re + lam_im * lam_im
        m_re, m_im = paired[0, k], paired[1, k]
        for b, value in enumerate(
            (
                (m_re * lam_re + m_im * lam_im) / size,
                (m_im * lam_re - m_re * lam_im) / size,
                paired[2, k],
                -paired[3, k],
            )
        ):
            at = (b // 2) * LANES + (2 * k + b % 2) * channels
            tables[me, at : at + channels, :] = value.astype(BF16)


def mixer_kernel(
    tokens, proj, decay, frequency, input_map, readout, step_hbm, in_gain_hbm, out_gain_hbm, shaped,
    tok, wide, tables, rates, steps, step, in_gain, out_gain,
    decay_in, frequency_in, input_map_in, readout_in, paired,
    normed, drive, q_re, q_im, g_re, g_im, inj, back, pushed, answer, tau,
    send1, got1, decays, plane_end, plane_got, plane_time, time_got, send3, got3,
    block_end, block_got, block_in,
    load, s1, r1, s2, r2, st, rt, s3, r3,
    proj_sent, proj_got, table_sent, table_got, rate_sent, rate_got, pass_sent, pass_got,
    sb, rb, ready, all_in,
):
    rows = tok.shape[0]
    tp_count, sp_count = lax.axis_size("tp"), lax.axis_size("sp")
    planes = sp_count // 2
    members = 2 * tp_count
    me, sp = lax.axis_index("tp"), lax.axis_index("sp")
    core, plane = lax.rem(sp, 2), sp // 2
    first = plane - lax.rem(plane, BLOCK)
    stop = jnp.minimum(first + BLOCK, planes)
    reach = jnp.where(plane == stop - 1, jnp.minimum(stop + BLOCK, planes), stop)
    place = core * tp_count + me
    tiles = q_re.shape[0]
    per_shard = tiles // tp_count
    shards = tp_count

    def member(k):
        return {"sp": plane * 2 + k // tp_count, "tp": k % tp_count}

    def at_plane(z):
        return {"sp": z * 2 + core}

    partner = {"sp": sp + 1 - 2 * core}

    def loop(lower, upper, body):
        def step(z, carry):
            body(z)
            return carry

        lax.fori_loop(lower, upper, step, 0)

    hub, gate = 1, 2
    first_chip = me == 0
    barrier = pltpu.get_barrier_semaphore()

    def greet(target):
        pl.semaphore_signal(barrier, inc=1, device_id=target, device_id_type=MESH)

    loads = [
        pltpu.make_async_copy(src, dst, load.at[k])
        for k, (src, dst) in enumerate(
            (
                (tokens, tok),
                (proj, wide.at[me]),
                (step_hbm, step),
                (in_gain_hbm, in_gain),
                (out_gain_hbm, out_gain),
            )
        )
    ]

    @pl.when(core == 1)
    def _():
        for k in range(1, tp_count):
            greet({"tp": lax.rem(me + k, tp_count)})

    @pl.when((core == 0) != first_chip)
    def _():
        greet(partner)

    @pl.when(place != hub)
    def _():
        greet(member(hub))

    for k in (2, 0, 1, 3, 4):
        loads[k].start()

    def plane_in():
        pl.semaphore_wait(barrier, members - 1)
        greet(member(gate))
        loop(jnp.maximum(first - 1, 0), plane, lambda z: greet({"sp": 2 * z, "tp": gate}))

    @pl.when(jnp.logical_and(place == hub, plane > 0))
    def _():
        plane_in()

    passed = [
        (rates, rates),
        (tables, tables),
        *((wide.at[lax.rem(me + k, tp_count)],) * 2 for k in range(1, tp_count)),
        (step, steps.at[1]),
    ]

    def pass_on(slot):
        src, dst = passed[slot]
        return pltpu.make_async_remote_copy(
            src_ref=src, dst_ref=dst, send_sem=pass_sent.at[slot], recv_sem=pass_got.at[slot],
            device_id=partner, device_id_type=MESH,
        )

    def pass_back():
        slot = len(passed)
        return pltpu.make_async_remote_copy(
            src_ref=step, dst_ref=steps.at[0], send_sem=pass_sent.at[slot],
            recv_sem=pass_got.at[slot], device_id=partner, device_id_type=MESH,
        )

    def pass_all():
        for slot in (0, *range(2, len(passed)), 1):
            pass_on(slot).start()

    @pl.when(core == 1)
    def _():
        inward = [
            pltpu.make_async_copy(src, dst, load.at[len(loads) + k])
            for k, (src, dst) in enumerate(
                (
                    (decay, decay_in),
                    (frequency, frequency_in),
                    (input_map, input_map_in),
                    (readout, readout_in),
                )
            )
        ]
        for copy in inward:
            copy.start()
        for copy in inward:
            copy.wait()
        own_tables(
            tables, rates, me, decay_in, frequency_in, input_map_in, readout_in, paired
        )
        loads[1].wait()
        pl.semaphore_wait(barrier, tp_count - jnp.where(first_chip, 1, 0))
        gather_over_tp(
            wide, tables, rates, proj_sent, proj_got, table_sent, table_got, rate_sent, rate_got
        )

    @pl.when(jnp.logical_and(core == 0, first_chip))
    def _():
        pl.semaphore_wait(barrier, 1)
        pl.semaphore_signal(ready, inc=1, device_id=partner, device_id_type=MESH)

    loads[2].wait()

    @pl.when(jnp.logical_and(core == 1, jnp.logical_not(first_chip)))
    def _():
        pass_all()

    row = lax.broadcasted_iota(jnp.int32, (rows, LANES), 0)
    lane = lax.broadcasted_iota(jnp.int32, (rows, LANES), 1)
    step_rows = rows // LANES
    column = jnp.zeros((rows, 1), F32)
    for k in range(step_rows):
        line = step[pl.ds(me * step_rows + k, 1), :]
        column += jnp.sum(
            jnp.where(lane + k * LANES <= row, jnp.broadcast_to(line, (rows, LANES)), 0.0),
            axis=1, keepdims=True,
        )
    tau[...] = jnp.broadcast_to(column, (rows, LANES))
    loads[0].wait()
    loads[3].wait()
    strip = rows // tiles

    def norm(i):
        here = pl.ds(pl.multiple_of(i * strip, strip), strip)
        value = tok[here, :].astype(F32)
        scale = lax.rsqrt(jnp.mean(value * value, axis=1, keepdims=True) + 1e-06)
        normed[here, :] = (value * scale * in_gain[...]).astype(BF16)

    @pl.when(core == 0)
    def _():
        pass_on(0).wait_recv()

    first_row = lax.broadcasted_iota(jnp.int32, (8, LANES), 0) == 0

    def rate_row(i):
        return rates[i // per_shard, pl.ds(lax.rem(i, per_shard), 1), :]

    def turn_rows(i):
        return turns_of(rates[i // per_shard, pl.ds(per_shard + lax.rem(i, per_shard), 1), :])

    def tables_of(i, carry):
        norm(i)
        rate, (high, low) = rate_row(i), turn_rows(i)
        before = [jnp.ones((8, LANES), F32), jnp.zeros((8, LANES), F32)]
        for c in range(0, rows, CHUNK):
            here = pl.ds(c, CHUNK)
            times = tau[here, :]
            grow = jnp.exp(rate * times)
            for b, (part, q_ref, g_ref) in enumerate(
                zip(rotation(high, low, times), (q_re, q_im), (g_re, g_im))
            ):
                value = grow * part
                q_ref[i, here, :] = value
                turned = pltpu.roll(value, 1, 0)
                head = jnp.where(first_row, before[b], turned[:8])
                before[b] = turned[:8]
                g_ref[i, here, :] = jnp.concatenate([head, turned[8:]], axis=0) - value
        return carry

    lax.fori_loop(0, tiles, tables_of, 0)

    @pl.when(core == 0)
    def _():
        loads[1].wait()
        for slot in range(1, len(passed)):
            pass_on(slot).wait_recv()

    for t in range(0, shards, 2):
        both = jnp.dot(
            normed[...],
            jnp.concatenate([wide[t], wide[t + 1]], axis=1),
            preferred_element_type=F32,
        )
        drive[t] = both[:, :LANES].astype(BF16)
        drive[t + 1] = both[:, LANES:].astype(BF16)

    k_row = lax.broadcasted_iota(jnp.int32, (LANES, LANES), 0)
    k_lane = lax.broadcasted_iota(jnp.int32, (LANES, LANES), 1)
    group_rows = LANES // (2 * per_shard)

    def own_groups(inner):
        return k_row // group_rows == 2 * inner + k_lane // (LANES // 2)

    def compact(shard, block):
        at = pl.multiple_of(block * group_rows, group_rows)
        return tables[shard, pl.ds(at, group_rows), :].astype(F32)

    def widened(value, mask):
        return jnp.where(mask, jnp.concatenate([value] * (LANES // group_rows), axis=0), 0.0).astype(
            BF16
        )

    def spread(shard, block, mask):
        return widened(compact(shard, block), mask)

    def push_through(i, half):
        shard, inner = i // per_shard, lax.rem(i, per_shard)
        mask = own_groups(inner)
        push = [spread(shard, 2 * inner + b, mask) for b in range(2)]
        pushed[half] = jnp.dot(
            drive[shard], jnp.concatenate(push, axis=1), preferred_element_type=F32
        )

    def inject(i, half):
        sum_re = jnp.zeros((CHUNK, LANES), F32)
        sum_im = jnp.zeros((CHUNK, LANES), F32)
        for c in range(0, rows, CHUNK):
            here = pl.ds(c, CHUNK)
            u_re, u_im = pushed[half, here, :LANES], pushed[half, here, LANES:]
            a_re, a_im = g_re[i, here, :], g_im[i, here, :]
            w_re = a_re * u_re - a_im * u_im
            w_im = a_re * u_im + a_im * u_re
            sum_re += w_re
            sum_im += w_im
            inj[i, here, :LANES] = w_re.astype(BF16)
            inj[i, here, LANES:] = w_im.astype(BF16)
        t_re = jnp.sum(sum_re, axis=0, keepdims=True)
        t_im = jnp.sum(sum_im, axis=0, keepdims=True)
        fade = jnp.exp(-2.0 * (rate_row(i) * tau[rows - 1 : rows, :]))
        d_re, d_im = q_re[i, rows - 1 : rows, :] * fade, -(q_im[i, rows - 1 : rows, :] * fade)
        part = i // 2
        send1[part, half : half + 1, :] = d_re * t_re - d_im * t_im
        send1[part, 2 + half : 3 + half, :] = d_re * t_im + d_im * t_re
        send1[part, 4 + half : 5 + half, :] = d_re
        send1[part, 6 + half : 7 + half, :] = d_im

    def inject_pair(part, carry):
        push_through(2 * part, 0)
        push_through(2 * part + 1, 1)
        inject(2 * part, 0)
        inject(2 * part + 1, 1)
        return carry

    lax.fori_loop(0, tiles // 2, inject_pair, 0)

    @pl.when(jnp.logical_and(core == 1, first_chip))
    def _():
        pl.semaphore_wait(ready, 1)
        pass_all()

    @pl.when(jnp.logical_and(place == hub, plane == 0))
    def _():
        plane_in()

    @pl.when(place == gate)
    def _():
        pl.semaphore_wait(barrier, reach - plane)
        for k in range(members):
            if k != gate:
                pl.semaphore_signal(all_in, inc=1, device_id=member(k), device_id_type=MESH)

    @pl.when(place != gate)
    def _():
        pl.semaphore_wait(all_in, 1)

    @pl.when(core == 0)
    def _():
        pass_back().start()

    def copy1(k):
        return pltpu.make_async_remote_copy(
            src_ref=send1.at[k], dst_ref=got1.at[place], send_sem=s1.at[k], recv_sem=r1.at[place],
            device_id=member(k), device_id_type=MESH,
        )

    for k in range(members):
        @pl.when(place != k)
        def _():
            copy1(k).start()

    def copy_time(z):
        return pltpu.make_async_remote_copy(
            src_ref=plane_time, dst_ref=time_got.at[plane], send_sem=st.at[z],
            recv_sem=rt.at[plane], device_id=at_plane(z), device_id_type=MESH,
        )

    @pl.when(core == 1)
    def _():
        pass_back().wait_recv()

    steps[pl.ds(core, 1)] = step[...].reshape(1, *step.shape)
    whole_plane = jnp.sum(jnp.sum(steps[0] + steps[1], axis=1, keepdims=True), axis=0, keepdims=True)
    plane_time[...] = jnp.broadcast_to(whole_plane, plane_time.shape)
    loop(plane + 1, stop, lambda z: copy_time(z).start())
    p_row = lax.broadcasted_iota(jnp.int32, (rows, rows), 0)
    p_col = lax.broadcasted_iota(jnp.int32, (rows, rows), 1)
    lower = jnp.where(p_col <= p_row, 1.0, 0.0).astype(BF16)

    blocks = LANES // group_rows

    def across(left, right):
        return lax.dot_general(
            left, right, (((1,), (1,)), ((), ())), preferred_element_type=F32
        )

    def prefix(i, slot, first):
        shard, inner = i // per_shard, lax.rem(i, per_shard)
        pushed[slot] = jnp.dot(lower, inj[i], preferred_element_type=F32)
        rate = rate_row(i)
        for c in range(0, rows, CHUNK):
            here = pl.ds(c, CHUNK)
            fade = jnp.exp(-2.0 * (rate * tau[here, :]))
            e_re, e_im = q_re[i, here, :] * fade, -(q_im[i, here, :] * fade)
            a_re, a_im = pushed[slot, here, :LANES], pushed[slot, here, LANES:]
            back[i, here, :LANES] = e_re.astype(BF16)
            back[i, here, LANES:] = e_im.astype(BF16)
            inj[i, here, :LANES] = (e_re * a_re - e_im * a_im).astype(BF16)
            inj[i, here, LANES:] = (e_re * a_im + e_im * a_re).astype(BF16)
        mask = own_groups(inner)
        read = [spread(shard, blocks + 2 * inner + b, mask) for b in range(2)]
        value = across(inj[i], jnp.concatenate(read, axis=1))
        if first:
            answer[shard] = value
        else:
            answer[shard] += value

    def prefixes(shard):
        for inner in range(per_shard):
            prefix(shard * per_shard + inner, inner % 2, inner == 0)

    got1[pl.ds(place, 1)] = send1[pl.ds(place, 1)]
    for k in range(members):
        @pl.when(place != k)
        def _():
            pltpu.make_async_remote_copy(
                src_ref=send1.at[k], dst_ref=got1.at[k], send_sem=s1.at[k], recv_sem=r1.at[k],
                device_id=member(k), device_id_type=MESH,
            ).wait_recv()

    def advance(k, re, im):
        block = got1[k]
        d_re, d_im = block[4:6], block[6:8]
        return d_re * re - d_im * im + block[0:2], d_re * im + d_im * re + block[2:4]

    nothing = jnp.zeros((2, LANES), F32)
    re, im = nothing, nothing
    for k in range(members):
        re, im = advance(k, re, im)
    plane_end[0:2, :] = re
    plane_end[2:4, :] = im

    def copy2(z):
        return pltpu.make_async_remote_copy(
            src_ref=plane_end, dst_ref=plane_got.at[plane], send_sem=s2.at[z],
            recv_sem=r2.at[plane], device_id=at_plane(z), device_id_type=MESH,
        )

    loop(plane + 1, stop, lambda z: copy2(z).start())

    @pl.when(plane > 0)
    def _():
        loop(0, shards, prefixes)

    def time_wait(z):
        pltpu.make_async_remote_copy(
            src_ref=plane_time, dst_ref=time_got.at[z], send_sem=st.at[z], recv_sem=rt.at[z],
            device_id=at_plane(z), device_id_type=MESH,
        ).wait_recv()

    loop(first, plane, time_wait)

    def plane_decay(z):
        times = jnp.broadcast_to(time_got[z], (1, LANES))
        for half in range(2):
            i = 2 * place + half
            rate, (high, low) = rate_row(i), turn_rows(i)
            cosine, sine = rotation(high, low, times)
            shrink = jnp.exp(-(rate * times))
            decays[z, half : half + 1, :] = shrink * cosine
            decays[z, 2 + half : 3 + half, :] = -(shrink * sine)

    loop(first, plane, plane_decay)

    def end_wait(z):
        pltpu.make_async_remote_copy(
            src_ref=plane_end, dst_ref=plane_got.at[z], send_sem=s2.at[z], recv_sem=r2.at[z],
            device_id=at_plane(z), device_id_type=MESH,
        ).wait_recv()

    loop(first, plane, end_wait)

    def earlier(z, carry):
        re, im = carry
        d, end = decays[z], plane_got[z]
        return (
            d[0:2] * re - d[2:4] * im + end[0:2],
            d[0:2] * im + d[2:4] * re + end[2:4],
        )

    def copy_block(z):
        return pltpu.make_async_remote_copy(
            src_ref=block_end, dst_ref=block_got, send_sem=sb.at[z], recv_sem=rb,
            device_id=at_plane(z), device_id_type=MESH,
        )

    @pl.when(first == 0)
    def _():
        block_in[...] = jnp.zeros_like(block_in)

    @pl.when(first > 0)
    def _():
        copy_block(plane).wait_recv()
        block_in[...] = block_got[...]

    re, im = lax.fori_loop(first, plane, earlier, (block_in[0:2, :], block_in[2:4, :]))

    @pl.when(reach > stop)
    def _():
        after_re, after_im = re, im
        for k in range(members):
            after_re, after_im = advance(k, after_re, after_im)
        block_end[0:2, :] = after_re
        block_end[2:4, :] = after_im

    loop(stop, reach, lambda z: copy_block(z).start())
    for k in range(members):
        send3[k, 0:2, :] = re
        send3[k, 2:4, :] = im
        if k < members - 1:
            re, im = advance(k, re, im)

    def copy3(k):
        return pltpu.make_async_remote_copy(
            src_ref=send3.at[k], dst_ref=got3.at[place], send_sem=s3.at[k], recv_sem=r3.at[place],
            device_id=member(k), device_id_type=MESH,
        )

    for k in range(members):
        @pl.when(place != k)
        def _():
            copy3(k).start()

    @pl.when(plane == 0)
    def _():
        loop(0, shards, prefixes)

    got3[pl.ds(place, 1)] = send3[pl.ds(place, 1)]
    for k in range(members):
        @pl.when(place != k)
        def _():
            pltpu.make_async_remote_copy(
                src_ref=send3.at[k], dst_ref=got3.at[k], send_sem=s3.at[k], recv_sem=r3.at[k],
                device_id=member(k), device_id_type=MESH,
            ).wait_recv()

    def respond(shard):
        value = answer[shard]
        for inner in range(per_shard):
            i = shard * per_shard + inner
            part, half = i // 2, inner % 2
            in_re = got3[part, half : half + 1, :]
            in_im = got3[part, 2 + half : 3 + half, :]
            c_re, c_im = (compact(shard, blocks + 2 * inner + b) for b in range(2))
            mask = own_groups(inner)
            read = [
                widened(c_re * in_re + c_im * in_im, mask),
                widened(c_im * in_re - c_re * in_im, mask),
            ]
            value += across(back[i], jnp.concatenate(read, axis=1))
        answer[shard] = value

    loop(0, shards, respond)

    loads[4].wait()

    def finish(i):
        here = pl.ds(pl.multiple_of(i * CHUNK, CHUNK), CHUNK)
        values = []
        squares = jnp.zeros((CHUNK, LANES), F32)
        for t in range(shards):
            v = answer[t, here, :]
            v = 0.5 * v * (1.0 + jnp.tanh(0.7978845608 * (v + 0.044715 * (v * v * v))))
            v = v.astype(BF16).astype(F32)
            values.append(v)
            squares += v * v
        mean = jnp.sum(squares, axis=1, keepdims=True) * np.float32(1.0 / (shards * LANES))
        scale = lax.rsqrt(mean + 1e-06)
        for t in range(shards):
            line = pl.ds(t * LANES, LANES)
            shaped[here, line] = (values[t] * scale * out_gain[:, line]).astype(BF16)

    loop(0, rows // CHUNK, finish)

    for k in range(members):
        @pl.when(place != k)
        def _():
            copy1(k).wait_send()
            copy3(k).wait_send()
    loop(plane + 1, stop, lambda z: copy_time(z).wait_send())
    loop(plane + 1, stop, lambda z: copy2(z).wait_send())
    loop(stop, reach, lambda z: copy_block(z).wait_send())

    @pl.when(core == 1)
    def _():
        for slot in range(len(passed)):
            pass_on(slot).wait_send()

    @pl.when(core == 0)
    def _():
        pass_back().wait_send()


def mix(tokens, proj, decay, frequency, input_map, readout, step, in_gain, out_gain):
    rows, width = tokens.shape
    shards = lax.axis_size("tp")
    planes = lax.axis_size("sp") // 2
    members = 2 * shards
    pairs = decay.size // LANES
    tiles = shards * pairs
    vmem = pl.BlockSpec(memory_space=pltpu.VMEM)
    far = pl.BlockSpec(memory_space=pltpu.HBM)
    table = pltpu.VMEM((tiles, rows, LANES), F32)
    dma = pltpu.SemaphoreType.DMA
    passed = shards + 3
    return pl.pallas_call(
        mixer_kernel,
        out_shape=jax.ShapeDtypeStruct((rows, shards * LANES), BF16),
        in_specs=[far] * 9,
        out_specs=vmem,
        scratch_shapes=[
            pltpu.VMEM(tokens.shape, BF16),
            pltpu.VMEM((shards, *proj.shape), BF16),
            pltpu.VMEM((shards, 2 * LANES, LANES), BF16),
            pltpu.VMEM((shards, 2 * pairs, LANES), F32),
            pltpu.VMEM((2, *step.shape), F32),
            *(pltpu.VMEM(a.shape, F32) for a in (step, in_gain, out_gain)),
            *(pltpu.VMEM(a.shape, F32) for a in (decay, frequency, input_map, readout)),
            pltpu.VMEM((4, pairs, input_map.shape[2], LANES), F32),
            pltpu.VMEM(tokens.shape, BF16),
            pltpu.VMEM((shards, rows, LANES), BF16),
            table, table, table, table,
            pltpu.VMEM((tiles, rows, 2 * LANES), BF16),
            pltpu.VMEM((tiles, rows, 2 * LANES), BF16),
            pltpu.VMEM((2, rows, 2 * LANES), F32),
            pltpu.VMEM((shards, rows, LANES), F32),
            pltpu.VMEM((rows, LANES), F32),
            pltpu.VMEM((members, 8, LANES), F32),
            pltpu.VMEM((members, 8, LANES), F32),
            pltpu.VMEM((planes, 4, LANES), F32),
            pltpu.VMEM((4, LANES), F32),
            pltpu.VMEM((planes, 4, LANES), F32),
            pltpu.VMEM((1, LANES), F32),
            pltpu.VMEM((planes, 1, LANES), F32),
            pltpu.VMEM((members, 4, LANES), F32),
            pltpu.VMEM((members, 4, LANES), F32),
            pltpu.VMEM((4, LANES), F32),
            pltpu.VMEM((4, LANES), F32),
            pltpu.VMEM((4, LANES), F32),
            dma((9,)),
            dma((members,)), dma((members,)),
            dma((planes,)), dma((planes,)),
            dma((planes,)), dma((planes,)),
            dma((members,)), dma((members,)),
            dma((6,)), dma((6,)), dma((6,)), dma((6,)), dma((3,)), dma((3,)),
            dma((passed,)), dma((passed,)),
            dma((planes,)), dma,
            pltpu.SemaphoreType.REGULAR,
            pltpu.SemaphoreType.REGULAR,
        ],
        compiler_params=pltpu.CompilerParams(
            collective_id=0, has_side_effects=True, vmem_limit_bytes=48 << 20
        ),
        name="mixer",
    )(
        *(
            pltpu.with_memory_space_constraint(a, pltpu.HBM)
            for a in (tokens, proj, decay, frequency, input_map, readout, step, in_gain, out_gain)
        )
    )


def on_device(
    tokens, step, in_gain, in_proj, decay_rate, frequency, input_map, readout, out_gain, out_proj
):
    shaped = mix(
        tokens, in_proj, decay_rate, frequency, jnp.swapaxes(input_map, 2, 3), readout,
        step.reshape(-1, LANES), in_gain.reshape(1, -1), out_gain.reshape(1, -1),
    )
    return jnp.dot(shaped, out_proj, preferred_element_type=F32).astype(BF16)


def solution(mesh):
    placed = (
        P(("grp", "sp", "tp"), None),
        P(("grp", "sp")),
        P(),
        P(None, "tp"),
        P("tp", None),
        P("tp", None),
        P(None, "tp", None, None),
        P(None, "tp", None, None),
        P(),
        P(),
    )
    return jax.shard_map(
        on_device,
        mesh=mesh,
        in_specs=placed,
        out_specs=P(("grp", "sp", "tp"), None),
        check_vma=False,
    )
```
